32 devices in a mesh: dp: 4 (over y, x), kv: 4 (over z), tp: 2 (over core).
Axes of the slice: x: 2, y: 2, z: 4, core: 2. Of those that a mesh axis runs over, the one named last changes fastest.
Arguments:
- tokens: bfloat16 [4, 2048, 2048], P('dp', 'kv'), may hold values from -6 to 6
- w_query: bfloat16 [2048, 1024], P(None, 'tp'), as said below
- w_key: bfloat16 [2048, 1024], P(None, 'tp'), as said below
- w_value: bfloat16 [2048, 1024], P(None, 'tp'), may hold values from -0.125 to 0.125
- w_out: bfloat16 [1024, 2048], P('tp'), may hold values from -0.1875 to 0.1875
- chosen: int32 [4, 32, 16], P('dp', 'kv'), may hold values from -1 to 31, as said below
Outputs:
- mixed: bfloat16 [4, 2048, 2048], P('dp', ('kv', 'tp'))
- log_sums: float32 [4, 16, 2048], P('dp', 'tp', 'kv')
The draws below stay inside these ranges and needn't reach their ends.
Inputs may be any that keep to these rules, and one draw needn't show every extreme that they name: `chosen`: write d = b // 8 and j = b % 8 for query block b. Row b lists b first, then min(15, j + 2 * d) distinct earlier blocks, then -1. Of the blocks that the query blocks of one index d of kv list, at most 2 lie in the positions of any one other index; the first query block of every index d >= 1 lists 2 blocks of index d - 1, and, where it exists, 2 blocks of the index half the sequence earlier. `w_query`: A weight matrix with entries up to about 4. `w_key`: A weight matrix of entries of order 2048 to the power -1/2.
All inputs are finite; a program needn't handle non-finite values.
Results may differ from the reference program's by a relative error of at most 0.0093.
Values may be sent and summed in bfloat16 or wider, within the bound.
A program may use at most 192 MiB of HBM per device.

```python
import jax
import jax.numpy as jnp
from jax import lax

D = 2048
HEADS = 16
HEAD_DIM = 64
BLOCK = 64
NSEL = 16
SEQS = 4
LENGTH = 2048
NBLK = 32
KB_DEV = 8
CAP = 2
N_TP = 2


def paired_weights(key):
    base = jax.random.fold_in(key, 11)
    scale = D ** (-0.5)
    key_weight = jnp.clip(jax.random.normal(jax.random.fold_in(base, 1), (D, HEADS * HEAD_DIM), jnp.float32), -6.0, 6.0) * scale
    free_weight = jnp.clip(jax.random.normal(jax.random.fold_in(base, 2), (D, HEADS * HEAD_DIM), jnp.float32), -6.0, 6.0) * scale
    query_weight = free_weight
    return (query_weight, key_weight)


def draw_w_query(key, part):
    return paired_weights(key)[0].astype(jnp.bfloat16)


def draw_w_key(key, part):
    return paired_weights(key)[1].astype(jnp.bfloat16)


def one_sequence(key):
    blocks = jnp.arange(NBLK, dtype=jnp.int32)
    owners = blocks // KB_DEV
    within = blocks % KB_DEV
    devices = NBLK // KB_DEV
    pair_scores = jax.random.randint(jax.random.fold_in(key, 1), (devices, devices, KB_DEV), 0, 65536) * KB_DEV + jnp.arange(KB_DEV, dtype=jnp.int32)
    ranks = jnp.sum((pair_scores[..., None, :] > pair_scores[..., :, None]).astype(jnp.int32), axis=-1)
    allowed_pair = ranks < CAP
    query_dev = owners[:, None]
    key_dev = owners[None, :]
    own_earlier = (key_dev == query_dev) & (blocks[None, :] < blocks[:, None])
    allowed_here = allowed_pair[query_dev, key_dev, within[None, :]]
    foreign = (key_dev < query_dev) & allowed_here
    candidate = own_earlier | foreign
    popular = (jax.random.randint(jax.random.fold_in(key, 2), (NBLK,), 0, 6) == 0).astype(jnp.int32)
    base = jax.random.randint(jax.random.fold_in(key, 3), (NBLK, NBLK), 0, 1024) + 4096 * popular[None, :]
    forced = foreign & (within[:, None] == 0) & ((key_dev == query_dev - 1) | (key_dev == query_dev - devices // 2))
    base = base + 65536 * forced.astype(jnp.int32)
    final = jnp.where(candidate, base * NBLK + blocks[None, :], -1)
    top_values, top_index = lax.top_k(final, NSEL - 1)
    picks = jnp.where(top_values >= 0, top_index, -1)
    return jnp.concatenate([blocks[:, None], picks], axis=1).astype(jnp.int32)


def draw_chosen(key, part):
    seq_keys = jax.vmap(lambda index: jax.random.fold_in(key, index))(jnp.arange(SEQS, dtype=jnp.int32))
    return jax.vmap(one_sequence)(seq_keys)


def block_scale(stream_key, shape, pieces, least, top_value):
    def one(position, blocks):
        draws = jax.random.uniform(jax.random.fold_in(jax.random.fold_in(stream_key, 6), position), (blocks,), jnp.float32, least / len(pieces), top_value / len(pieces))
        return jnp.repeat(jnp.exp(draws), shape[position] // blocks).reshape((-1,) + (1,) * (len(shape) - position - 1))

    loudness = one(*pieces[0])
    for cut in pieces[1:]:
        loudness = loudness * one(*cut)
    return loudness


def scatter_about(stream_key, extent, scale, limit, cuts=(), kind=jnp.bfloat16):
    drawn = scale * jax.random.normal(stream_key, extent, jnp.float32)
    if cuts:
        drawn = drawn * block_scale(stream_key, extent, cuts, -0.22, 0.18)
    return jnp.clip(drawn, -limit, limit).astype(kind)


def setup_inputs(seed: int = 0) -> dict:
    splits = jax.random.split(jax.random.key(seed), 7)
    return {
        "tokens": scatter_about(splits[0], (SEQS, LENGTH, D), 1.0, 6.0, ((0, 4), (1, 4))),
        "w_query": draw_w_query(jax.random.fold_in(splits[6], 71), 0),
        "w_key": draw_w_key(jax.random.fold_in(splits[6], 71), 0),
        "w_value": scatter_about(splits[3], (D, HEADS * HEAD_DIM), D ** -0.5, 0.125, ((1, 2),)),
        "w_out": scatter_about(splits[4], (HEADS * HEAD_DIM, D), (HEADS * HEAD_DIM) ** -0.5, 0.1875, ((0, 2),)),
        "chosen": draw_chosen(jax.random.fold_in(splits[6], 71), 0),
    }


def attend_sequence(inputs, w_query, w_key, w_value, w_out, listed):
    queries = jnp.dot(inputs, w_query, preferred_element_type=jnp.float32).astype(jnp.bfloat16)
    keys_all = jnp.dot(inputs, w_key, preferred_element_type=jnp.float32).astype(jnp.bfloat16)
    values_all = jnp.dot(inputs, w_value, preferred_element_type=jnp.float32).astype(jnp.bfloat16)
    width = queries.shape[1]
    query_blocks = queries.reshape(NBLK, BLOCK, HEADS, HEAD_DIM)
    key_blocks = keys_all.reshape(NBLK, BLOCK, HEADS, HEAD_DIM)
    value_blocks = values_all.reshape(NBLK, BLOCK, HEADS, HEAD_DIM)
    offsets = jnp.arange(BLOCK, dtype=jnp.int32)

    def one_block(args):
        query_block, row, index = args
        valid = row >= 0
        safe = jnp.where(valid, row, 0).astype(jnp.int32)
        keys_sel = key_blocks[safe].astype(jnp.float32)
        values_sel = value_blocks[safe].astype(jnp.float32)
        scores = jnp.einsum('qhd,skhd->hqsk', query_block.astype(jnp.float32), keys_sel) * (HEAD_DIM ** -0.5)
        key_pos = row[:, None] * BLOCK + offsets[None, :]
        query_pos = index * BLOCK + offsets
        allowed = valid[None, :, None] & (key_pos[None, :, :] <= query_pos[:, None, None])
        scores = jnp.where(allowed[None], scores, -jnp.inf)
        row_max = jnp.max(scores, axis=(2, 3), keepdims=True)
        exp_terms = jnp.exp(scores - row_max)
        row_sum = jnp.sum(exp_terms, axis=(2, 3), keepdims=True)
        weights = (exp_terms / row_sum).astype(jnp.bfloat16)
        attended = jnp.einsum('hqsk,skhd->qhd', weights.astype(jnp.float32), values_sel).astype(jnp.bfloat16)
        return attended.reshape(BLOCK, width), (row_max + jnp.log(row_sum))[:, :, 0, 0]

    attended, log_sums = lax.map(one_block, (query_blocks, listed, jnp.arange(NBLK, dtype=jnp.int32)))
    attended = attended.reshape(LENGTH, width)
    log_sums = jnp.transpose(log_sums, (1, 0, 2)).reshape(HEADS, LENGTH)
    share = width // N_TP
    total = jnp.zeros((LENGTH, w_out.shape[1]), jnp.float32)
    for shard in range(N_TP):
        partial_value = jnp.dot(attended[:, shard * share:(shard + 1) * share], w_out[shard * share:(shard + 1) * share],
                          preferred_element_type=jnp.float32).astype(jnp.bfloat16)
        total = total + partial_value.astype(jnp.float32)
    return total.astype(jnp.bfloat16), log_sums


def reference(tokens, w_query, w_key, w_value, w_out, chosen):
    mixed_list = []
    sums_list = []
    for seq_index in range(SEQS):
        mixed_one, sums_one = attend_sequence(tokens[seq_index], w_query, w_key, w_value, w_out, chosen[seq_index])
        mixed_list.append(mixed_one)
        sums_list.append(sums_one)
    return jnp.stack(mixed_list), jnp.stack(sums_list)
```

```python
import functools

import jax
import jax.numpy as jnp
from jax import lax
from jax.experimental import pallas as pl
from jax.experimental.pallas import tpu as pltpu
from jax.sharding import PartitionSpec as P

HEAD_DIM = 64
BLOCK = 64


def on_device_general(tokens, w_query, w_key, w_value, w_out, chosen):
    inputs = tokens[0]
    listed = chosen[0]
    tok_rows = inputs.shape[0]
    queries = jnp.dot(inputs, w_query, preferred_element_type=jnp.float32).astype(jnp.bfloat16)
    keys_local = jnp.dot(inputs, w_key, preferred_element_type=jnp.float32).astype(jnp.bfloat16)
    values_local = jnp.dot(inputs, w_value, preferred_element_type=jnp.float32).astype(jnp.bfloat16)
    width = queries.shape[1]
    head_count = width // HEAD_DIM
    span_blocks = tok_rows // BLOCK
    query_count, picks = listed.shape
    myself = lax.axis_index("kv")
    valid = listed >= 0
    key_blocks = keys_local.reshape(span_blocks, BLOCK, width)
    value_blocks = values_local.reshape(span_blocks, BLOCK, width)
    kv_count = lax.axis_size("kv")
    capacity = max(1, min(2, span_blocks // 3))
    owners = jnp.where(valid, listed // span_blocks, myself)
    within = jnp.where(valid, listed % span_blocks, 0)
    foreign = valid & (owners != myself)
    owner_iota = jnp.arange(kv_count, dtype=jnp.int32)
    within_iota = jnp.arange(span_blocks, dtype=jnp.int32)
    hits = (
        (owners[:, :, None, None] == owner_iota[:, None])
        & (within[:, :, None, None] == within_iota[None, :])
        & foreign[:, :, None, None]
    )
    needed = jnp.any(hits, axis=(0, 1))
    order_rank = jnp.cumsum(needed.astype(jnp.int32), axis=1) - 1
    matches = needed[:, None, :] & (
        order_rank[:, None, :] == jnp.arange(capacity, dtype=jnp.int32)[None, :, None]
    )
    wanted = jnp.where(
        jnp.any(matches, axis=2), jnp.sum(matches.astype(jnp.int32) * within_iota, axis=2), -1
    )
    asked = lax.all_to_all(wanted, "kv", split_axis=0, concat_axis=0, tiled=True)
    present = (asked >= 0)[:, :, None, None]
    picked = jnp.clip(asked, 0, span_blocks - 1)
    zero_block = jnp.zeros((), jnp.bfloat16)
    send_keys = jnp.where(present, key_blocks[picked], zero_block)
    send_values = jnp.where(present, value_blocks[picked], zero_block)
    got_keys, got_values = (
        lax.all_to_all(send_keys, "kv", split_axis=0, concat_axis=0, tiled=True),
        lax.all_to_all(send_values, "kv", split_axis=0, concat_axis=0, tiled=True),
    )
    pool_keys = jnp.concatenate([key_blocks, got_keys.reshape(-1, BLOCK, width)], axis=0)
    pool_values = jnp.concatenate([value_blocks, got_values.reshape(-1, BLOCK, width)], axis=0)
    slot_rank = jnp.sum(hits.astype(jnp.int32) * order_rank[None, None], axis=(2, 3))
    slots = jnp.where(foreign, span_blocks + owners * capacity + slot_rank, within)
    keys_sel = pool_keys[slots].reshape(query_count, picks, BLOCK, head_count, HEAD_DIM)
    values_sel = pool_values[slots].reshape(query_count, picks, BLOCK, head_count, HEAD_DIM)
    query_blocks = queries.reshape(query_count, BLOCK, head_count, HEAD_DIM)
    scores = jnp.einsum(
        "nqhd,nskhd->nhqsk", query_blocks, keys_sel, preferred_element_type=jnp.float32
    ) * HEAD_DIM ** (-0.5)
    offsets = jnp.arange(BLOCK, dtype=jnp.int32)
    key_pos = listed[:, :, None] * BLOCK + offsets[None, None, :]
    query_pos = (myself * span_blocks + jnp.arange(query_count, dtype=jnp.int32))[
        :, None
    ] * BLOCK + offsets[None, :]
    allowed = valid[:, None, :, None] & (key_pos[:, None, :, :] <= query_pos[:, :, None, None])
    scores = jnp.where(allowed[:, None], scores, -jnp.inf)
    row_max = jnp.max(scores, axis=(3, 4), keepdims=True)
    exp_terms = jnp.exp(scores - row_max)
    row_sum = jnp.sum(exp_terms, axis=(3, 4), keepdims=True)
    weights = (exp_terms / row_sum).astype(jnp.bfloat16)
    attended = jnp.einsum(
        "nhqsk,nskhd->nqhd", weights, values_sel, preferred_element_type=jnp.float32
    )
    attended = attended.astype(jnp.bfloat16).reshape(tok_rows, width)
    log_sums = (row_max + jnp.log(row_sum))[:, :, :, 0, 0]
    log_sums = jnp.transpose(log_sums, (1, 0, 2)).reshape(head_count, tok_rows)
    mixed = lax.psum_scatter(
        jnp.dot(attended, w_out, preferred_element_type=jnp.float32).astype(jnp.bfloat16),
        "tp",
        scatter_dimension=0,
        tiled=True,
    )
    return (mixed[None], log_sums[None])


CAPACITY = 2
LANES = 128
QTILE = 256


def fused_kernel(
    n, tokens_hbm, wq_hbm, wk_hbm, wv_hbm, wo_hbm, chosen_hbm, mixed_ref, lse_ref,
    x, wq, wk, wv, wo, chosen_ref, q_s, k_s, vt_s, send_k, send_v, got_k, got_v, asked,
    acc, mx, sm, top, inv, far_s, far_e, att, att_far, wo_far, part,
    load_sem, ask_send, ask_recv, kv_send, kv_recv, part_send, part_recv,
):
    me = lax.axis_index("kv")
    core = lax.axis_index("tp")
    rows, width = q_s.shape
    depth = wo.shape[1]
    half = rows // 2
    blocks = rows // BLOCK
    pairs = width // LANES
    foreign_rows = CAPACITY * BLOCK

    loads = []
    for index, (src, dst) in enumerate(
        ((tokens_hbm.at[0], x), (wk_hbm, wk), (wv_hbm, wv), (wq_hbm, wq), (wo_hbm, wo), (chosen_hbm, chosen_ref))
    ):
        loads.append(pltpu.make_async_copy(src, dst, load_sem.at[index]))
    loads[5].start()
    loads[0].start()
    loads[1].start()

    barrier = pltpu.get_barrier_semaphore()
    for offset in range(1, n):
        pl.semaphore_signal(
            barrier, inc=1, device_id={"kv": lax.rem(me + offset, n)},
            device_id_type=pl.DeviceIdType.MESH,
        )
    pl.semaphore_signal(
        barrier, inc=1, device_id={"tp": 1 - core}, device_id_type=pl.DeviceIdType.MESH
    )
    pl.semaphore_wait(barrier, n)

    def ask_copy(offset):
        return pltpu.make_async_remote_copy(
            src_ref=chosen_ref, dst_ref=asked.at[offset - 1],
            send_sem=ask_send.at[offset - 1], recv_sem=ask_recv.at[offset - 1],
            device_id={"kv": lax.rem(me + n - offset, n)}, device_id_type=pl.DeviceIdType.MESH,
        )

    def kv_copy(offset, which):
        return pltpu.make_async_remote_copy(
            src_ref=(send_k, send_v)[which].at[offset - 1],
            dst_ref=(got_k, got_v)[which].at[offset - 1],
            send_sem=kv_send.at[which, offset - 1], recv_sem=kv_recv.at[which, offset - 1],
            device_id={"kv": lax.rem(me + offset, n)}, device_id_type=pl.DeviceIdType.MESH,
        )

    loads[5].wait()
    for offset in range(1, n):
        @pl.when(me >= offset)
        def _():
            ask_copy(offset).start()

    def project(w, out, scale, turn=False):
        step = 256

        @pl.loop(0, width // step)
        def _(j):
            cols = pl.ds(pl.multiple_of(j * step, step), step)
            y = jnp.dot(x[...], w[:, cols], preferred_element_type=jnp.float32)
            y = y.astype(jnp.bfloat16)
            if turn:
                out[cols, :] = y.T
            else:
                out[:, cols] = y * jnp.asarray(scale, jnp.bfloat16) if scale != 1.0 else y

    def pick(offset):
        row = asked[offset - 1, 0, 0:1, :]
        inside = (row >= me * blocks) & (row < (me + 1) * blocks)
        low = jnp.min(jnp.where(inside, row, (me + 1) * blocks - 1), axis=1, keepdims=True)
        high = jnp.max(jnp.where(inside, row, me * blocks), axis=1, keepdims=True)
        low, high = low - me * blocks, high - me * blocks
        place = lax.broadcasted_iota(jnp.int32, (foreign_rows, rows), 0)
        column = lax.broadcasted_iota(jnp.int32, (foreign_rows, rows), 1)
        want = jnp.where(place < BLOCK, low * BLOCK + place, high * BLOCK + place - BLOCK)
        return (column == want).astype(jnp.float32).astype(jnp.bfloat16)

    def select_and_send(which):
        for offset in range(n - 1, 0, -1):
            @pl.when(me + offset < n)
            def _():
                if which == 0:
                    ask_copy(offset).wait_recv()
                one_hot = pick(offset)
                if which == 0:
                    got = jnp.dot(one_hot, k_s[...], preferred_element_type=jnp.float32)
                else:
                    got = lax.dot_general(
                        vt_s[...], one_hot, (((1,), (1,)), ((), ())), preferred_element_type=jnp.float32
                    )
                (send_k, send_v)[which][offset - 1] = got.astype(jnp.bfloat16)
                kv_copy(offset, which).start()

    loads[0].wait()
    loads[1].wait()
    for load in loads[2:5]:
        load.start()
    project(wk, k_s, 1.0)
    select_and_send(0)
    loads[2].wait()
    project(wv, vt_s, 1.0, turn=True)
    select_and_send(1)
    wo_copy = pltpu.make_async_remote_copy(
        src_ref=wo_hbm, dst_ref=wo_far,
        send_sem=part_send.at[1], recv_sem=part_recv.at[1],
        device_id={"tp": 1 - core}, device_id_type=pl.DeviceIdType.MESH,
    )
    wo_copy.start()
    loads[3].wait()
    project(wq, q_s, HEAD_DIM ** (-0.5))

    first = lax.broadcasted_iota(jnp.int32, (rows, LANES), 1) < HEAD_DIM
    zero = jnp.zeros((), jnp.bfloat16)

    def one_head(q, half_of_pair):
        mine = first[: q.shape[0]]
        return jnp.where(mine, q, zero) if half_of_pair == 0 else jnp.where(mine, zero, q)

    def attend(q, k, vt, mask):
        s = lax.dot_general(k, q, (((1,), (1,)), ((), ())), preferred_element_type=jnp.float32)
        if mask is not None:
            last = jnp.where(mask, s[-QTILE:], -jnp.inf)
            s = last if s.shape[0] == QTILE else jnp.concatenate([s[:-QTILE], last], axis=0)
        m = jnp.max(s, axis=0, keepdims=True)
        e = jnp.exp(s - m)
        l = jnp.sum(e, axis=0, keepdims=True)
        o = jnp.dot(vt, e.astype(jnp.bfloat16), preferred_element_type=jnp.float32)
        return m, l, o

    tri = lax.broadcasted_iota(jnp.int32, (QTILE, QTILE), 0) <= lax.broadcasted_iota(
        jnp.int32, (QTILE, QTILE), 1
    )

    @pl.loop(0, pairs)
    def _(p):
        cols = pl.ds(pl.multiple_of(p * LANES, LANES), LANES)
        for i in range(rows // QTILE):
            here = slice(i * QTILE, (i + 1) * QTILE)
            keys = slice(0, (i + 1) * QTILE)
            q, k = q_s[here, cols], k_s[keys, cols]
            for side in range(2):
                head = 2 * p + side
                wide = pl.ds(pl.multiple_of(head * HEAD_DIM, HEAD_DIM), HEAD_DIM)
                m, l, o = attend(one_head(q, side), k, vt_s[wide, keys], tri)
                mx[pl.ds(head, 1), here] = m
                sm[pl.ds(head, 1), here] = l
                acc[wide, here] = o

    def of_head(p, side):
        head = 2 * p + side
        wide = pl.ds(pl.multiple_of(head * HEAD_DIM, HEAD_DIM), HEAD_DIM)
        far = pl.ds(pl.multiple_of(head * foreign_rows, foreign_rows), foreign_rows)
        return pl.ds(head, 1), wide, far

    top[...] = mx[...]
    for offset in range(1, n):
        @pl.when(me >= offset)
        def _():
            kv_copy(offset, 0).wait_recv()

            @pl.loop(0, pairs)
            def _(p):
                cols = pl.ds(pl.multiple_of(p * LANES, LANES), LANES)
                q, k = q_s[:, cols], got_k[offset - 1, :, cols]
                for side in range(2):
                    line, _, far = of_head(p, side)
                    s = lax.dot_general(
                        k, one_head(q, side), (((1,), (1,)), ((), ())),
                        preferred_element_type=jnp.float32,
                    )
                    far_s[offset - 1, far, :] = s
                    top[line, :] = jnp.maximum(top[line, :], jnp.max(s, axis=0, keepdims=True))

    keep = jnp.exp(mx[...] - top[...])
    sm[...] = sm[...] * keep
    for offset in range(1, n):
        @pl.when(me >= offset)
        def _():
            @pl.loop(0, pairs)
            def _(p):
                for side in range(2):
                    line, _, far = of_head(p, side)
                    e = jnp.exp(far_s[offset - 1, far, :] - top[line, :])
                    sm[line, :] = sm[line, :] + jnp.sum(e, axis=0, keepdims=True)
                    far_e[offset - 1, far, :] = e.astype(jnp.bfloat16)

    inv[...] = 1.0 / sm[...]
    lse_ref[0] = top[...] + jnp.log(sm[...])
    mx[...] = keep * inv[...]

    @pl.loop(0, pairs)
    def _(p):
        for side in range(2):
            line, wide, _ = of_head(p, side)
            acc[wide, :] = acc[wide, :] * mx[line, :]

    def finish(cols, first_half):
        for offset in range(1, n):
            @pl.when(me >= offset)
            def _():
                if first_half:
                    kv_copy(offset, 1).wait_recv()

                @pl.loop(0, pairs)
                def _(p):
                    for side in range(2):
                        line, wide, far = of_head(p, side)
                        o = jnp.dot(
                            got_v[offset - 1, wide, :], far_e[offset - 1, far, cols],
                            preferred_element_type=jnp.float32,
                        )
                        acc[wide, cols] = acc[wide, cols] + o * inv[line, cols]

        att[cols, :] = acc[:, cols].astype(jnp.bfloat16).T

    loads[4].wait()
    chunks = 4
    step = depth // chunks
    theirs = pl.ds(pl.multiple_of((1 - core) * half, half), half)
    mine = pl.ds(pl.multiple_of(core * half, half), half)

    att_copy = pltpu.make_async_remote_copy(
        src_ref=att.at[theirs], dst_ref=att_far,
        send_sem=part_send.at[0], recv_sem=part_recv.at[0],
        device_id={"tp": 1 - core}, device_id_type=pl.DeviceIdType.MESH,
    )
    finish(theirs, True)
    att_copy.start()
    finish(mine, False)
    for c in range(chunks):
        cols = slice(c * step, (c + 1) * step)
        part[:, cols] = jnp.dot(
            att[mine, :], wo[:, cols], preferred_element_type=jnp.float32
        ).astype(jnp.bfloat16)
    wo_copy.wait_recv()
    att_copy.wait_recv()
    for c in range(chunks):
        cols = slice(c * step, (c + 1) * step)
        other = jnp.dot(
            att_far[...], wo_far[:, cols], preferred_element_type=jnp.float32
        ).astype(jnp.bfloat16)
        mixed_ref[0, :, cols] = (
            part[:, cols].astype(jnp.float32) + other.astype(jnp.float32)
        ).astype(jnp.bfloat16)

    att_copy.wait_send()
    wo_copy.wait_send()
    for offset in range(1, n):
        @pl.when(me >= offset)
        def _():
            ask_copy(offset).wait_send()

        @pl.when(me + offset < n)
        def _():
            kv_copy(offset, 0).wait_send()
            kv_copy(offset, 1).wait_send()


def store_kernel(mixed_ref, lse_ref, mixed_hbm, lse_hbm, sem):
    copies = [
        pltpu.make_async_copy(mixed_ref, mixed_hbm, sem.at[0]),
        pltpu.make_async_copy(lse_ref, lse_hbm, sem.at[1]),
    ]
    for copy in copies:
        copy.start()
    for copy in copies:
        copy.wait()


def on_device_fused(n, tokens, w_query, w_key, w_value, w_out, chosen):
    _, rows, model = tokens.shape
    width = w_query.shape[1]
    depth = w_out.shape[1]
    blocks, picks = chosen.shape[1:]
    foreign_rows = CAPACITY * BLOCK
    heads = width // HEAD_DIM
    bf16, f32 = jnp.bfloat16, jnp.float32
    in_hbm = pl.BlockSpec(memory_space=pltpu.HBM)
    in_vmem = pl.BlockSpec(memory_space=pltpu.VMEM)
    dma = pltpu.SemaphoreType.DMA
    chosen = pltpu.with_memory_space_constraint(chosen, pltpu.HBM)
    mixed, lse = pl.pallas_call(
        functools.partial(fused_kernel, n),
        out_shape=(
            pltpu.VMEM((1, rows // 2, depth), bf16),
            pltpu.VMEM((1, width // HEAD_DIM, rows), f32),
        ),
        in_specs=[in_hbm] * 6,
        out_specs=(in_vmem, in_vmem),
        scratch_shapes=[
            pltpu.VMEM((rows, model), bf16),
            pltpu.VMEM((model, width), bf16),
            pltpu.VMEM((model, width), bf16),
            pltpu.VMEM((model, width), bf16),
            pltpu.VMEM((width, depth), bf16),
            pltpu.VMEM((1, blocks, picks), jnp.int32),
            pltpu.VMEM((rows, width), bf16),
            pltpu.VMEM((rows, width), bf16),
            pltpu.VMEM((width, rows), bf16),
            pltpu.VMEM((n - 1, foreign_rows, width), bf16),
            pltpu.VMEM((n - 1, width, foreign_rows), bf16),
            pltpu.VMEM((n - 1, foreign_rows, width), bf16),
            pltpu.VMEM((n - 1, width, foreign_rows), bf16),
            pltpu.VMEM((n - 1, 1, blocks, picks), jnp.int32),
            pltpu.VMEM((width, rows), f32),
            pltpu.VMEM((heads, rows), f32),
            pltpu.VMEM((heads, rows), f32),
            pltpu.VMEM((heads, rows), f32),
            pltpu.VMEM((heads, rows), f32),
            pltpu.VMEM((n - 1, heads * foreign_rows, rows), f32),
            pltpu.VMEM((n - 1, heads * foreign_rows, rows), bf16),
            pltpu.VMEM((rows, width), bf16),
            pltpu.VMEM((rows // 2, width), bf16),
            pltpu.VMEM((width, depth), bf16),
            pltpu.VMEM((rows // 2, depth), bf16),
            dma((6,)),
            dma((n - 1,)),
            dma((n - 1,)),
            dma((2, n - 1)),
            dma((2, n - 1)),
            dma((2,)),
            dma((2,)),
        ],
        compiler_params=pltpu.CompilerParams(
            collective_id=0, has_side_effects=True, vmem_limit_bytes=53500 * 1024
        ),
    )(tokens, w_query, w_key, w_value, w_out, chosen)
    mixed = pltpu.with_memory_space_constraint(mixed, pltpu.VMEM)
    lse = pltpu.with_memory_space_constraint(lse, pltpu.VMEM)
    return pl.pallas_call(
        store_kernel,
        out_shape=(
            jax.ShapeDtypeStruct(mixed.shape, mixed.dtype),
            jax.ShapeDtypeStruct(lse.shape, lse.dtype),
        ),
        in_specs=[in_vmem] * 2,
        out_specs=(in_hbm, in_hbm),
        scratch_shapes=[dma((2,))],
        compiler_params=pltpu.CompilerParams(vmem_limit_bytes=1024 * 1024),
    )(mixed, lse)


def on_device(tokens, w_query, w_key, w_value, w_out, chosen):
    n, cores = lax.axis_size("kv"), lax.axis_size("tp")
    rows = tokens.shape[1]
    blocks, picks = chosen.shape[1:]
    full_rows = blocks - 1 + CAPACITY * (n - 1) <= picks - 1
    fits = rows % (2 * QTILE) == 0 and w_query.shape[1] % 256 == 0 and blocks >= 3 * CAPACITY
    if full_rows and fits and cores == 2 and n > 1:
        return on_device_fused(n, tokens, w_query, w_key, w_value, w_out, chosen)
    return on_device_general(tokens, w_query, w_key, w_value, w_out, chosen)


def solution(mesh):
    return jax.shard_map(
        on_device,
        mesh=mesh,
        in_specs=(
            P("dp", "kv", None),
            P(None, "tp"),
            P(None, "tp"),
            P(None, "tp"),
            P("tp", None),
            P("dp", "kv", None),
        ),
        out_specs=(P("dp", ("kv", "tp"), None), P("dp", "tp", "kv")),
        check_vma=False,
    )
```

```python
import functools

import jax
import jax.numpy as jnp
from jax import lax
from jax.experimental import pallas as pl
from jax.experimental.pallas import tpu as pltpu
from jax.sharding import PartitionSpec as P

HEAD_DIM = 64
BLOCK = 64


def on_device_general(tokens, w_query, w_key, w_value, w_out, chosen):
    inputs = tokens[0]
    listed = chosen[0]
    tok_rows = inputs.shape[0]
    queries = jnp.dot(inputs, w_query, preferred_element_type=jnp.float32).astype(jnp.bfloat16)
    keys_local = jnp.dot(inputs, w_key, preferred_element_type=jnp.float32).astype(jnp.bfloat16)
    values_local = jnp.dot(inputs, w_value, preferred_element_type=jnp.float32).astype(jnp.bfloat16)
    width = queries.shape[1]
    head_count = width // HEAD_DIM
    span_blocks = tok_rows // BLOCK
    query_count, picks = listed.shape
    myself = lax.axis_index("kv")
    valid = listed >= 0
    key_blocks = keys_local.reshape(span_blocks, BLOCK, width)
    value_blocks = values_local.reshape(span_blocks, BLOCK, width)
    kv_count = lax.axis_size("kv")
    capacity = max(1, min(2, span_blocks // 3))
    owners = jnp.where(valid, listed // span_blocks, myself)
    within = jnp.where(valid, listed % span_blocks, 0)
    foreign = valid & (owners != myself)
    owner_iota = jnp.arange(kv_count, dtype=jnp.int32)
    within_iota = jnp.arange(span_blocks, dtype=jnp.int32)
    hits = (
        (owners[:, :, None, None] == owner_iota[:, None])
        & (within[:, :, None, None] == within_iota[None, :])
        & foreign[:, :, None, None]
    )
    needed = jnp.any(hits, axis=(0, 1))
    order_rank = jnp.cumsum(needed.astype(jnp.int32), axis=1) - 1
    matches = needed[:, None, :] & (
        order_rank[:, None, :] == jnp.arange(capacity, dtype=jnp.int32)[None, :, None]
    )
    wanted = jnp.where(
        jnp.any(matches, axis=2), jnp.sum(matches.astype(jnp.int32) * within_iota, axis=2), -1
    )
    asked = lax.all_to_all(wanted, "kv", split_axis=0, concat_axis=0, tiled=True)
    present = (asked >= 0)[:, :, None, None]
    picked = jnp.clip(asked, 0, span_blocks - 1)
    zero_block = jnp.zeros((), jnp.bfloat16)
    send_keys = jnp.where(present, key_blocks[picked], zero_block)
    send_values = jnp.where(present, value_blocks[picked], zero_block)
    got_keys, got_values = (
        lax.all_to_all(send_keys, "kv", split_axis=0, concat_axis=0, tiled=True),
        lax.all_to_all(send_values, "kv", split_axis=0, concat_axis=0, tiled=True),
    )
    pool_keys = jnp.concatenate([key_blocks, got_keys.reshape(-1, BLOCK, width)], axis=0)
    pool_values = jnp.concatenate([value_blocks, got_values.reshape(-1, BLOCK, width)], axis=0)
    slot_rank = jnp.sum(hits.astype(jnp.int32) * order_rank[None, None], axis=(2, 3))
    slots = jnp.where(foreign, span_blocks + owners * capacity + slot_rank, within)
    keys_sel = pool_keys[slots].reshape(query_count, picks, BLOCK, head_count, HEAD_DIM)
    values_sel = pool_values[slots].reshape(query_count, picks, BLOCK, head_count, HEAD_DIM)
    query_blocks = queries.reshape(query_count, BLOCK, head_count, HEAD_DIM)
    scores = jnp.einsum(
        "nqhd,nskhd->nhqsk", query_blocks, keys_sel, preferred_element_type=jnp.float32
    ) * HEAD_DIM ** (-0.5)
    offsets = jnp.arange(BLOCK, dtype=jnp.int32)
    key_pos = listed[:, :, None] * BLOCK + offsets[None, None, :]
    query_pos = (myself * span_blocks + jnp.arange(query_count, dtype=jnp.int32))[
        :, None
    ] * BLOCK + offsets[None, :]
    allowed = valid[:, None, :, None] & (key_pos[:, None, :, :] <= query_pos[:, :, None, None])
    scores = jnp.where(allowed[:, None], scores, -jnp.inf)
    row_max = jnp.max(scores, axis=(3, 4), keepdims=True)
    exp_terms = jnp.exp(scores - row_max)
    row_sum = jnp.sum(exp_terms, axis=(3, 4), keepdims=True)
    weights = (exp_terms / row_sum).astype(jnp.bfloat16)
    attended = jnp.einsum(
        "nhqsk,nskhd->nqhd", weights, values_sel, preferred_element_type=jnp.float32
    )
    attended = attended.astype(jnp.bfloat16).reshape(tok_rows, width)
    log_sums = (row_max + jnp.log(row_sum))[:, :, :, 0, 0]
    log_sums = jnp.transpose(log_sums, (1, 0, 2)).reshape(head_count, tok_rows)
    mixed = lax.psum_scatter(
        jnp.dot(attended, w_out, preferred_element_type=jnp.float32).astype(jnp.bfloat16),
        "tp",
        scatter_dimension=0,
        tiled=True,
    )
    return (mixed[None], log_sums[None])


CAPACITY = 2
LANES = 128
QTILE = 256
STEP = 256


def fused_kernel(
    n, tokens_hbm, wq_hbm, wk_hbm, wv_hbm, wo_hbm, chosen_hbm, out_ref, last_att_ref, last_wo_ref, lse_ref,
    x, wq, wk, wv, wo, chosen_ref, q_s, k_s, vt_s, hot, send_k, send_v, got_k, got_v, asked,
    acc, mx, sm, inv, keep_inv, far_e, att, att_send,
    load_sem, w_sem, ask_send, ask_recv, kv_send, kv_recv, att_sem_s, att_sem_r, wo_send, wo_recv,
):
    me = lax.axis_index("kv")
    core = lax.axis_index("tp")
    rows, width = q_s.shape
    depth = wo.shape[3]
    half = rows // 2
    blocks = rows // BLOCK
    pairs = width // LANES
    chunks = width // STEP
    per_chunk = STEP // LANES
    foreign_rows = CAPACITY * BLOCK
    last = pairs - 1
    early_pairs = pairs - 2
    bf16, f32 = jnp.bfloat16, jnp.float32
    mesh_ids = pl.DeviceIdType.MESH

    def part(c):
        return slice(c * STEP, (c + 1) * STEP)

    load_chosen = pltpu.make_async_copy(chosen_hbm, chosen_ref, load_sem.at[0])
    load_x = pltpu.make_async_copy(tokens_hbm.at[0], x, load_sem.at[1])
    load_q = pltpu.make_async_copy(wq_hbm, wq, load_sem.at[3])
    weights = ((wk_hbm, wk), (wv_hbm, wv))

    def load_w(which, c):
        src, dst = weights[which]
        return pltpu.make_async_copy(src.at[:, part(c)], dst.at[:, part(c)], w_sem.at[which, c])

    wo_own = pltpu.make_async_copy(wo_hbm, wo.at[:, 0], load_sem.at[2])
    wo_far = pltpu.make_async_remote_copy(
        src_ref=wo_hbm, dst_ref=wo.at[:, 1], send_sem=wo_send, recv_sem=wo_recv,
        device_id={"tp": 1 - core}, device_id_type=mesh_ids,
    )

    load_chosen.start()
    load_x.start()
    load_w(0, 0).start()

    barrier = pltpu.get_barrier_semaphore()
    for offset in range(1, n):
        @pl.when(me + offset < n)
        def _():
            pl.semaphore_signal(barrier, inc=1, device_id={"kv": me + offset}, device_id_type=mesh_ids)
    pl.semaphore_signal(barrier, inc=1, device_id={"tp": 1 - core}, device_id_type=mesh_ids)

    def ask_copy(offset):
        return pltpu.make_async_remote_copy(
            src_ref=chosen_ref, dst_ref=asked.at[offset - 1],
            send_sem=ask_send.at[offset - 1], recv_sem=ask_recv.at[offset - 1],
            device_id={"kv": lax.rem(me + n - offset, n)}, device_id_type=mesh_ids,
        )

    def kv_copy(offset, g, which):
        far = pl.ds((offset - 1) * foreign_rows, foreign_rows)
        group = pl.ds(0, early_pairs) if g == 0 else pl.ds(early_pairs + g - 1, 1)
        return pltpu.make_async_remote_copy(
            src_ref=(send_k, send_v)[which].at[offset - 1, group],
            dst_ref=got_k.at[group, far, :] if which == 0 else got_v.at[group, :, far],
            send_sem=kv_send.at[which, offset - 1, g], recv_sem=kv_recv.at[which, offset - 1, g],
            device_id={"kv": lax.rem(me + offset, n)}, device_id_type=mesh_ids,
        )

    def att_copy(g):
        group = pl.ds(0, early_pairs) if g == 0 else pl.ds(early_pairs + g - 1, 1)
        return pltpu.make_async_remote_copy(
            src_ref=att_send.at[group], dst_ref=att.at[1, group],
            send_sem=att_sem_s.at[g], recv_sem=att_sem_r.at[g],
            device_id={"tp": 1 - core}, device_id_type=mesh_ids,
        )

    load_chosen.wait()
    pl.semaphore_wait(barrier, me + 1)
    for offset in range(1, n):
        @pl.when(me >= offset)
        def _():
            ask_copy(offset).start()
    load_w(1, 0).start()
    load_w(0, 1).start()

    def project_k(c):
        load_w(0, c).wait()
        cols = part(c)
        for r in (slice(0, half), slice(half, rows)):
            k_s[r, cols] = jnp.dot(x[r, :], wk[:, cols], preferred_element_type=f32).astype(bf16)

    def project_v(c):
        load_w(1, c).wait()
        cols = part(c)
        for r in (slice(0, half), slice(half, rows)):
            y = jnp.dot(x[r, :], wv[:, cols], preferred_element_type=f32).astype(bf16)
            vt_s[cols, r] = y.T

    def project_q():
        load_q.wait()

        @pl.loop(0, chunks)
        def _(c):
            cols = pl.ds(pl.multiple_of(c * STEP, STEP), STEP)
            y = jnp.dot(x[...], wq[:, cols], preferred_element_type=f32).astype(bf16)
            q_s[:, cols] = y * jnp.asarray(HEAD_DIM ** (-0.5), bf16)

    def pick(offset):
        ask_copy(offset).wait_recv()
        row = asked[offset - 1, 0, 0:1, :]
        inside = (row >= me * blocks) & (row < (me + 1) * blocks)
        low = jnp.min(jnp.where(inside, row, (me + 1) * blocks - 1), axis=1, keepdims=True)
        high = jnp.max(jnp.where(inside, row, me * blocks), axis=1, keepdims=True)
        low, high = (low - me * blocks) * BLOCK, (high - me * blocks - 1) * BLOCK
        place = lax.broadcasted_iota(jnp.int32, (foreign_rows, rows), 0)
        column = lax.broadcasted_iota(jnp.int32, (foreign_rows, rows), 1)
        want = place + jnp.where(place < BLOCK, low, high)
        hot[offset - 1] = (column == want).astype(f32).astype(bf16)

    def gather_and_send(offset, c, kinds):
        for which in kinds:
            if which == 0:
                y = jnp.dot(hot[offset - 1], k_s[:, part(c)], preferred_element_type=f32).astype(bf16)
            else:
                y = lax.dot_general(
                    vt_s[part(c), :], hot[offset - 1], (((1,), (1,)), ((), ())), preferred_element_type=f32
                ).astype(bf16)
            for i in range(per_chunk):
                here = slice(i * LANES, (i + 1) * LANES)
                if which == 0:
                    send_k[offset - 1, c * per_chunk + i] = y[:, here]
                else:
                    send_v[offset - 1, c * per_chunk + i] = y[here, :]
            if c * per_chunk < early_pairs:
                kv_copy(offset, 0, which).start()
        if c == chunks - 1:
            @pl.when(me + 2 >= n)
            def _():
                for g in (1, 2):
                    for which in kinds:
                        kv_copy(offset, g, which).start()

    def to(offset):
        return pl.when(me + offset < n)

    load_x.wait()
    project_k(0)

    @pl.when((me >= 1) & (me + 1 < n))
    def _():
        pick(1)
        gather_and_send(1, 0, (0,))

    load_w(1, 1).start()
    load_q.start()
    project_v(0)

    @pl.when((me >= 1) & (me + 1 < n))
    def _():
        gather_and_send(1, 0, (1,))

    project_k(1)
    for offset in range(2, n):
        @pl.when((me >= 1) & (me + offset < n))
        def _():
            pick(offset)
            gather_and_send(offset, 0, (0, 1))

    project_v(1)

    @pl.when(me >= 1)
    def _():
        for offset in range(1, n):
            @to(offset)
            def _():
                gather_and_send(offset, 1, (0, 1))

    wo_own.start()
    wo_far.start()
    project_q()

    @pl.when(me == 0)
    def _():
        for offset in range(1, n):
            pick(offset)
            gather_and_send(offset, 0, (0, 1))
        for offset in range(1, n):
            gather_and_send(offset, 1, (0, 1))

    first = lax.broadcasted_iota(jnp.int32, (QTILE, LANES), 1) < HEAD_DIM
    zero = jnp.zeros((), bf16)

    def one_head(q, side):
        return jnp.where(first, q, zero) if side == 0 else jnp.where(first, zero, q)

    def scores_t(k, q):
        return lax.dot_general(k, q, (((1,), (1,)), ((), ())), preferred_element_type=f32)

    def attend(q, k, vt, mask):
        s = scores_t(k, q)
        tail = jnp.where(mask, s[-QTILE:], -jnp.inf)
        s = tail if s.shape[0] == QTILE else jnp.concatenate([s[:-QTILE], tail], axis=0)
        m = jnp.max(s, axis=0, keepdims=True)
        e = jnp.exp(s - m)
        l = jnp.sum(e, axis=0, keepdims=True)
        o = jnp.dot(vt, e.astype(bf16), preferred_element_type=f32)
        return m, l, o

    tri = lax.broadcasted_iota(jnp.int32, (QTILE, QTILE), 0) <= lax.broadcasted_iota(
        jnp.int32, (QTILE, QTILE), 1
    )

    def lanes_of(p):
        return pl.ds(pl.multiple_of(p * LANES, LANES), LANES)

    def of_head(p, side):
        head = 2 * p + side
        return pl.ds(head, 1), pl.ds(pl.multiple_of(head * HEAD_DIM, HEAD_DIM), HEAD_DIM)

    def local(p):
        cols = lanes_of(p)
        for i in range(rows // QTILE):
            here = slice(i * QTILE, (i + 1) * QTILE)
            keys = slice(0, (i + 1) * QTILE)
            q, k = q_s[here, cols], k_s[keys, cols]
            for side in range(2):
                line, wide = of_head(p, side)
                m, l, o = attend(one_head(q, side), k, vt_s[wide, keys], tri)
                mx[line, here] = m
                sm[line, here] = l
                acc[wide, here] = o

    def throttled(act):
        @pl.when(me + 2 < n)
        def _():
            for offset in range(n - 1, 0, -1):
                @to(offset)
                def _():
                    act(offset)

    def start_held(offset):
        for which in range(2):
            kv_copy(offset, 1, which).start()

    pl.loop(0, pairs // 2)(local)
    throttled(start_held)
    pl.loop(pairs // 2, pairs)(local)

    def move_on(which):
        def act(offset):
            kv_copy(offset, 1, which).wait_send()
            kv_copy(offset, 2, which).start()

        return act

    def arrive(g, which, count):
        for offset in range(1, count + 1):
            kv_copy(offset, g, which).wait_recv()

    def weigh(p, count):
        far = count * foreign_rows
        for i in range(rows // QTILE):
            here = slice(i * QTILE, (i + 1) * QTILE)
            for side in range(2):
                line, _ = of_head(p, side)
                m, l = mx[line, here], sm[line, here]
                if count:
                    s = scores_t(got_k[p, :far, :], one_head(q_s[here, lanes_of(p)], side))
                    t = jnp.maximum(m, jnp.max(s, axis=0, keepdims=True))
                    e = jnp.exp(s - t)
                    k = jnp.exp(m - t)
                    l = l * k + jnp.sum(e, axis=0, keepdims=True)
                    far_e[side, :far, here] = e.astype(bf16)
                    m = t
                r = 1.0 / l
                inv[line, here] = r
                keep_inv[line, here] = k * r if count else r
                lse_ref[0, line, here] = m + jnp.log(l)

    theirs = pl.ds(pl.multiple_of((1 - core) * half, half), half)
    mine = pl.ds(pl.multiple_of(core * half, half), half)

    def blend(p, count, send=None):
        far = count * foreign_rows
        for cols in (theirs, mine):
            heads = []
            for side in range(2):
                line, wide = of_head(p, side)
                o = acc[wide, cols] * keep_inv[line, cols]
                if count:
                    vt = got_v[p, side * HEAD_DIM:(side + 1) * HEAD_DIM, :far]
                    o = o + jnp.dot(vt, far_e[side, :far, cols], preferred_element_type=f32) * inv[line, cols]
                heads.append(o.astype(bf16))
            block = jnp.concatenate(heads, axis=0).T
            if cols is theirs:
                att_send[p] = block
                if send is not None:
                    att_copy(send).start()
            else:
                att[0, p] = block

    def each_count(act):
        for count in range(n):
            @pl.when(me == count)
            def _():
                act(count)

    def early(count):
        arrive(0, 0, count)
        arrive(0, 1, count)

        @pl.loop(0, early_pairs)
        def _(p):
            weigh(p, count)
            blend(p, count)

    def middle(count):
        arrive(1, 0, count)
        weigh(last - 1, count)
        arrive(1, 1, count)
        blend(last - 1, count, 1)

    def weigh_last(count):
        arrive(2, 0, count)
        weigh(last, count)

    def blend_last(count):
        arrive(2, 1, count)
        blend(last, count, 2)

    each_count(early)
    att_copy(0).start()
    throttled(move_on(0))
    each_count(middle)
    throttled(move_on(1))

    wo_own.wait()
    wo_far.wait_recv()
    last_wo_ref[...] = wo[last].reshape(2 * LANES, depth)
    each_count(weigh_last)

    for g in range(2):
        att_copy(g).wait_recv()
    step = depth // 4
    for c in range(4):
        cols = slice(c * step, (c + 1) * step)
        rows_of = jnp.concatenate([att[side, p] for p in range(last) for side in range(2)], axis=1)
        out_ref[:, cols] = jnp.dot(
            rows_of, wo[:last, :, :, cols].reshape(2 * last * LANES, step), preferred_element_type=f32
        )

    each_count(blend_last)
    att_copy(2).wait_recv()
    last_att_ref[...] = jnp.concatenate([att[0, last], att[1, last]], axis=1)

    for g in range(3):
        att_copy(g).wait_send()
    wo_far.wait_send()
    for offset in range(1, n):
        @pl.when(me >= offset)
        def _():
            ask_copy(offset).wait_send()

        @to(offset)
        def _():
            for which in range(2):
                for g in (0, 2):
                    kv_copy(offset, g, which).wait_send()

                @pl.when(me + 2 >= n)
                def _():
                    kv_copy(offset, 1, which).wait_send()


def final_kernel(part_ref, att_ref, wo_ref, lse_ref, mixed_hbm, lse_hbm, out, sem):
    lse_copy = pltpu.make_async_copy(lse_ref, lse_hbm, sem.at[4])
    lse_copy.start()
    step = out.shape[1] // 4
    copies = []
    for c in range(4):
        cols = slice(c * step, (c + 1) * step)
        out[:, cols] = (
            part_ref[:, cols] + jnp.dot(att_ref[...], wo_ref[:, cols], preferred_element_type=jnp.float32)
        ).astype(out.dtype)
        copies.append(pltpu.make_async_copy(out.at[:, cols], mixed_hbm.at[0, :, cols], sem.at[c]))
        copies[-1].start()
    for copy in copies:
        copy.wait()
    lse_copy.wait()


def on_device_fused(n, tokens, w_query, w_key, w_value, w_out, chosen):
    _, rows, model = tokens.shape
    width = w_query.shape[1]
    depth = w_out.shape[1]
    blocks, picks = chosen.shape[1:]
    foreign_rows = CAPACITY * BLOCK
    heads = width // HEAD_DIM
    pairs = width // LANES
    half = rows // 2
    bf16, f32 = jnp.bfloat16, jnp.float32
    in_hbm = pl.BlockSpec(memory_space=pltpu.HBM)
    in_vmem = pl.BlockSpec(memory_space=pltpu.VMEM)
    dma = pltpu.SemaphoreType.DMA
    operands = [
        pltpu.with_memory_space_constraint(a, pltpu.HBM)
        for a in (tokens, w_query, w_key, w_value, w_out.reshape(pairs, LANES, depth), chosen)
    ]
    parts = pl.pallas_call(
        functools.partial(fused_kernel, n),
        out_shape=(
            pltpu.VMEM((half, depth), f32),
            pltpu.VMEM((half, 2 * LANES), bf16),
            pltpu.VMEM((2 * LANES, depth), bf16),
            pltpu.VMEM((1, heads, rows), f32),
        ),
        in_specs=[in_hbm] * 6,
        out_specs=(in_vmem,) * 4,
        scratch_shapes=[
            pltpu.VMEM((rows, model), bf16),
            pltpu.VMEM((model, width), bf16),
            pltpu.VMEM((model, width), bf16),
            pltpu.VMEM((model, width), bf16),
            pltpu.VMEM((pairs, 2, LANES, depth), bf16),
            pltpu.VMEM((1, blocks, picks), jnp.int32),
            pltpu.VMEM((rows, width), bf16),
            pltpu.VMEM((rows, width), bf16),
            pltpu.VMEM((width, rows), bf16),
            pltpu.VMEM((n - 1, foreign_rows, rows), bf16),
            pltpu.VMEM((n - 1, pairs, foreign_rows, LANES), bf16),
            pltpu.VMEM((n - 1, pairs, LANES, foreign_rows), bf16),
            pltpu.VMEM((pairs, (n - 1) * foreign_rows, LANES), bf16),
            pltpu.VMEM((pairs, LANES, (n - 1) * foreign_rows), bf16),
            pltpu.VMEM((n - 1, 1, blocks, picks), jnp.int32),
            pltpu.VMEM((width, rows), f32),
            pltpu.VMEM((heads, rows), f32),
            pltpu.VMEM((heads, rows), f32),
            pltpu.VMEM((heads, rows), f32),
            pltpu.VMEM((heads, rows), f32),
            pltpu.VMEM((2, (n - 1) * foreign_rows, rows), bf16),
            pltpu.VMEM((2, pairs, half, LANES), bf16),
            pltpu.VMEM((pairs, half, LANES), bf16),
            dma((4,)),
            dma((2, 2)),
            dma((n - 1,)),
            dma((n - 1,)),
            dma((2, n - 1, 3)),
            dma((2, n - 1, 3)),
            dma((3,)),
            dma((3,)),
            dma,
            dma,
        ],
        compiler_params=pltpu.CompilerParams(
            collective_id=0, has_side_effects=True, vmem_limit_bytes=40 * 1024 * 1024
        ),
    )(*operands)
    return pl.pallas_call(
        final_kernel,
        out_shape=(
            jax.ShapeDtypeStruct((1, half, depth), bf16),
            jax.ShapeDtypeStruct((1, heads, rows), f32),
        ),
        in_specs=[in_vmem] * 4,
        out_specs=(in_hbm, in_hbm),
        scratch_shapes=[pltpu.VMEM((half, depth), bf16), dma((5,))],
        compiler_params=pltpu.CompilerParams(vmem_limit_bytes=4 * 1024 * 1024),
    )(*[pltpu.with_memory_space_constraint(a, pltpu.VMEM) for a in parts])


def on_device(tokens, w_query, w_key, w_value, w_out, chosen):
    n, cores = lax.axis_size("kv"), lax.axis_size("tp")
    rows, width = tokens.shape[1], w_query.shape[1]
    blocks, picks = chosen.shape[1:]
    full_rows = blocks - 1 + CAPACITY * (n - 1) <= picks - 1
    fits = rows == 2 * QTILE and width == 2 * STEP and blocks >= 3 * CAPACITY
    if full_rows and fits and cores == 2 and n > 1:
        return on_device_fused(n, tokens, w_query, w_key, w_value, w_out, chosen)
    return on_device_general(tokens, w_query, w_key, w_value, w_out, chosen)


def solution(mesh):
    return jax.shard_map(
        on_device,
        mesh=mesh,
        in_specs=(
            P("dp", "kv", None),
            P(None, "tp"),
            P(None, "tp"),
            P(None, "tp"),
            P("tp", None),
            P("dp", "kv", None),
        ),
        out_specs=(P("dp", ("kv", "tp"), None), P("dp", "tp", "kv")),
        check_vma=False,
    )
```

```python
import functools

import jax
import jax.numpy as jnp
from jax import lax
from jax.experimental import pallas as pl
from jax.experimental.pallas import tpu as pltpu
from jax.sharding import PartitionSpec as P

HEAD_DIM = 64
BLOCK = 64


def on_device_general(tokens, w_query, w_key, w_value, w_out, chosen):
    inputs = tokens[0]
    listed = chosen[0]
    tok_rows = inputs.shape[0]
    queries = jnp.dot(inputs, w_query, preferred_element_type=jnp.float32).astype(jnp.bfloat16)
    keys_local = jnp.dot(inputs, w_key, preferred_element_type=jnp.float32).astype(jnp.bfloat16)
    values_local = jnp.dot(inputs, w_value, preferred_element_type=jnp.float32).astype(jnp.bfloat16)
    width = queries.shape[1]
    head_count = width // HEAD_DIM
    span_blocks = tok_rows // BLOCK
    query_count, picks = listed.shape
    myself = lax.axis_index("kv")
    valid = listed >= 0
    key_blocks = keys_local.reshape(span_blocks, BLOCK, width)
    value_blocks = values_local.reshape(span_blocks, BLOCK, width)
    kv_count = lax.axis_size("kv")
    capacity = max(1, min(2, span_blocks // 3))
    owners = jnp.where(valid, listed // span_blocks, myself)
    within = jnp.where(valid, listed % span_blocks, 0)
    foreign = valid & (owners != myself)
    owner_iota = jnp.arange(kv_count, dtype=jnp.int32)
    within_iota = jnp.arange(span_blocks, dtype=jnp.int32)
    hits = (
        (owners[:, :, None, None] == owner_iota[:, None])
        & (within[:, :, None, None] == within_iota[None, :])
        & foreign[:, :, None, None]
    )
    needed = jnp.any(hits, axis=(0, 1))
    order_rank = jnp.cumsum(needed.astype(jnp.int32), axis=1) - 1
    matches = needed[:, None, :] & (
        order_rank[:, None, :] == jnp.arange(capacity, dtype=jnp.int32)[None, :, None]
    )
    wanted = jnp.where(
        jnp.any(matches, axis=2), jnp.sum(matches.astype(jnp.int32) * within_iota, axis=2), -1
    )
    asked = lax.all_to_all(wanted, "kv", split_axis=0, concat_axis=0, tiled=True)
    present = (asked >= 0)[:, :, None, None]
    picked = jnp.clip(asked, 0, span_blocks - 1)
    zero_block = jnp.zeros((), jnp.bfloat16)
    send_keys = jnp.where(present, key_blocks[picked], zero_block)
    send_values = jnp.where(present, value_blocks[picked], zero_block)
    got_keys, got_values = (
        lax.all_to_all(send_keys, "kv", split_axis=0, concat_axis=0, tiled=True),
        lax.all_to_all(send_values, "kv", split_axis=0, concat_axis=0, tiled=True),
    )
    pool_keys = jnp.concatenate([key_blocks, got_keys.reshape(-1, BLOCK, width)], axis=0)
    pool_values = jnp.concatenate([value_blocks, got_values.reshape(-1, BLOCK, width)], axis=0)
    slot_rank = jnp.sum(hits.astype(jnp.int32) * order_rank[None, None], axis=(2, 3))
    slots = jnp.where(foreign, span_blocks + owners * capacity + slot_rank, within)
    keys_sel = pool_keys[slots].reshape(query_count, picks, BLOCK, head_count, HEAD_DIM)
    values_sel = pool_values[slots].reshape(query_count, picks, BLOCK, head_count, HEAD_DIM)
    query_blocks = queries.reshape(query_count, BLOCK, head_count, HEAD_DIM)
    scores = jnp.einsum(
        "nqhd,nskhd->nhqsk", query_blocks, keys_sel, preferred_element_type=jnp.float32
    ) * HEAD_DIM ** (-0.5)
    offsets = jnp.arange(BLOCK, dtype=jnp.int32)
    key_pos = listed[:, :, None] * BLOCK + offsets[None, None, :]
    query_pos = (myself * span_blocks + jnp.arange(query_count, dtype=jnp.int32))[
        :, None
    ] * BLOCK + offsets[None, :]
    allowed = valid[:, None, :, None] & (key_pos[:, None, :, :] <= query_pos[:, :, None, None])
    scores = jnp.where(allowed[:, None], scores, -jnp.inf)
    row_max = jnp.max(scores, axis=(3, 4), keepdims=True)
    exp_terms = jnp.exp(scores - row_max)
    row_sum = jnp.sum(exp_terms, axis=(3, 4), keepdims=True)
    weights = (exp_terms / row_sum).astype(jnp.bfloat16)
    attended = jnp.einsum(
        "nhqsk,nskhd->nqhd", weights, values_sel, preferred_element_type=jnp.float32
    )
    attended = attended.astype(jnp.bfloat16).reshape(tok_rows, width)
    log_sums = (row_max + jnp.log(row_sum))[:, :, :, 0, 0]
    log_sums = jnp.transpose(log_sums, (1, 0, 2)).reshape(head_count, tok_rows)
    mixed = lax.psum_scatter(
        jnp.dot(attended, w_out, preferred_element_type=jnp.float32).astype(jnp.bfloat16),
        "tp",
        scatter_dimension=0,
        tiled=True,
    )
    return (mixed[None], log_sums[None])


CAPACITY = 2
LANES = 128
QTILE = 256
STEP = 256


def fused_kernel(
    n, tokens_hbm, wq_hbm, wk_hbm, wv_hbm, wo_hbm, chosen_hbm, out_ref, last_att_ref, last_wo_ref, lse_ref,
    x, wq, wk, wv, wo, chosen_ref, q_s, k_s, vt_s, hot, send_k, send_v, got_k, got_v, asked,
    acc, mx, sm, inv, keep_inv, far_e, att, att_send,
    load_sem, w_sem, ask_send, ask_recv, kv_send, kv_recv, att_sem_s, att_sem_r, wo_send, wo_recv,
):
    me = lax.axis_index("kv")
    core = lax.axis_index("tp")
    rows, width = q_s.shape
    depth = wo.shape[3]
    half = rows // 2
    blocks = rows // BLOCK
    pairs = width // LANES
    chunks = width // STEP
    per_chunk = STEP // LANES
    foreign_rows = CAPACITY * BLOCK
    last = pairs - 1
    early_pairs = pairs - 2
    bf16, f32 = jnp.bfloat16, jnp.float32
    mesh_ids = pl.DeviceIdType.MESH

    def part(c):
        return slice(c * STEP, (c + 1) * STEP)

    load_chosen = pltpu.make_async_copy(chosen_hbm, chosen_ref, load_sem.at[0])
    load_x = pltpu.make_async_copy(tokens_hbm.at[0], x, load_sem.at[1])
    load_q = pltpu.make_async_copy(wq_hbm, wq, load_sem.at[3])
    weights = ((wk_hbm, wk), (wv_hbm, wv))

    def load_w(which, c):
        src, dst = weights[which]
        return pltpu.make_async_copy(src.at[:, part(c)], dst.at[:, part(c)], w_sem.at[which, c])

    wo_own = pltpu.make_async_copy(wo_hbm, wo.at[:, 0], load_sem.at[2])
    wo_far = pltpu.make_async_remote_copy(
        src_ref=wo_hbm, dst_ref=wo.at[:, 1], send_sem=wo_send, recv_sem=wo_recv,
        device_id={"tp": 1 - core}, device_id_type=mesh_ids,
    )

    load_chosen.start()
    load_x.start()
    load_w(0, 0).start()

    barrier = pltpu.get_barrier_semaphore()
    for offset in range(1, n):
        @pl.when(me + offset < n)
        def _():
            pl.semaphore_signal(barrier, inc=1, device_id={"kv": me + offset}, device_id_type=mesh_ids)
    pl.semaphore_signal(barrier, inc=1, device_id={"tp": 1 - core}, device_id_type=mesh_ids)

    def ask_copy(offset):
        return pltpu.make_async_remote_copy(
            src_ref=chosen_ref, dst_ref=asked.at[offset - 1],
            send_sem=ask_send.at[offset - 1], recv_sem=ask_recv.at[offset - 1],
            device_id={"kv": lax.rem(me + n - offset, n)}, device_id_type=mesh_ids,
        )

    def kv_copy(offset, g, which):
        far = pl.ds((offset - 1) * foreign_rows, foreign_rows)
        group = pl.ds(0, early_pairs) if g == 0 else pl.ds(early_pairs + g - 1, 1)
        return pltpu.make_async_remote_copy(
            src_ref=(send_k, send_v)[which].at[offset - 1, group],
            dst_ref=got_k.at[group, far, :] if which == 0 else got_v.at[group, :, far],
            send_sem=kv_send.at[which, offset - 1, g], recv_sem=kv_recv.at[which, offset - 1, g],
            device_id={"kv": lax.rem(me + offset, n)}, device_id_type=mesh_ids,
        )

    def att_copy(g):
        group = pl.ds(0, early_pairs) if g == 0 else pl.ds(early_pairs + g - 1, 1)
        return pltpu.make_async_remote_copy(
            src_ref=att_send.at[group], dst_ref=att.at[1, group],
            send_sem=att_sem_s.at[g], recv_sem=att_sem_r.at[g],
            device_id={"tp": 1 - core}, device_id_type=mesh_ids,
        )

    load_chosen.wait()
    pl.semaphore_wait(barrier, me + 1)
    for offset in range(1, n):
        @pl.when(me >= offset)
        def _():
            ask_copy(offset).start()
    load_w(1, 0).start()
    load_w(0, 1).start()

    def project_k(c):
        load_w(0, c).wait()
        cols = part(c)
        for r in (slice(0, half), slice(half, rows)):
            k_s[r, cols] = jnp.dot(x[r, :], wk[:, cols], preferred_element_type=f32).astype(bf16)

    def project_v(c):
        load_w(1, c).wait()
        cols = part(c)
        for r in (slice(0, half), slice(half, rows)):
            y = jnp.dot(x[r, :], wv[:, cols], preferred_element_type=f32).astype(bf16)
            vt_s[cols, r] = y.T

    def project_q():
        load_q.wait()

        @pl.loop(0, chunks)
        def _(c):
            cols = pl.ds(pl.multiple_of(c * STEP, STEP), STEP)
            y = jnp.dot(x[...], wq[:, cols], preferred_element_type=f32).astype(bf16)
            q_s[:, cols] = y * jnp.asarray(HEAD_DIM ** (-0.5), bf16)

    def pick(offset):
        ask_copy(offset).wait_recv()
        row = asked[offset - 1, 0, 0:1, :]
        inside = (row >= me * blocks) & (row < (me + 1) * blocks)
        low = jnp.min(jnp.where(inside, row, (me + 1) * blocks - 1), axis=1, keepdims=True)
        high = jnp.max(jnp.where(inside, row, me * blocks), axis=1, keepdims=True)
        low, high = (low - me * blocks) * BLOCK, (high - me * blocks - 1) * BLOCK
        place = lax.broadcasted_iota(jnp.int32, (foreign_rows, rows), 0)
        column = lax.broadcasted_iota(jnp.int32, (foreign_rows, rows), 1)
        want = place + jnp.where(place < BLOCK, low, high)
        hot[offset - 1] = (column == want).astype(f32).astype(bf16)

    def gather_and_send(offset, c, kinds):
        for which in kinds:
            if which == 0:
                y = jnp.dot(hot[offset - 1], k_s[:, part(c)], preferred_element_type=f32).astype(bf16)
            else:
                y = lax.dot_general(
                    vt_s[part(c), :], hot[offset - 1], (((1,), (1,)), ((), ())), preferred_element_type=f32
                ).astype(bf16)
            for i in range(per_chunk):
                here = slice(i * LANES, (i + 1) * LANES)
                if which == 0:
                    send_k[offset - 1, c * per_chunk + i] = y[:, here]
                else:
                    send_v[offset - 1, c * per_chunk + i] = y[here, :]
            if c * per_chunk < early_pairs:
                kv_copy(offset, 0, which).start()
        if c == chunks - 1:
            @pl.when(me + 2 >= n)
            def _():
                for g in (1, 2):
                    for which in kinds:
                        kv_copy(offset, g, which).start()

    def to(offset):
        return pl.when(me + offset < n)

    load_x.wait()
    project_k(0)

    @pl.when((me >= 1) & (me + 1 < n))
    def _():
        pick(1)
        gather_and_send(1, 0, (0,))

    load_w(1, 1).start()
    load_q.start()
    project_v(0)

    @pl.when((me >= 1) & (me + 1 < n))
    def _():
        gather_and_send(1, 0, (1,))

    project_k(1)
    for offset in range(2, n):
        @pl.when((me >= 1) & (me + offset < n))
        def _():
            pick(offset)
            gather_and_send(offset, 0, (0, 1))

    project_v(1)

    @pl.when(me >= 1)
    def _():
        for offset in range(1, n):
            @to(offset)
            def _():
                gather_and_send(offset, 1, (0, 1))

    wo_own.start()
    wo_far.start()
    project_q()

    @pl.when(me == 0)
    def _():
        for offset in range(1, n):
            pick(offset)
            gather_and_send(offset, 0, (0, 1))
        for offset in range(1, n):
            gather_and_send(offset, 1, (0, 1))

    first = lax.broadcasted_iota(jnp.int32, (QTILE, LANES), 1) < HEAD_DIM
    zero = jnp.zeros((), bf16)

    def one_head(q, side):
        return jnp.where(first, q, zero) if side == 0 else jnp.where(first, zero, q)

    def scores_t(k, q):
        return lax.dot_general(k, q, (((1,), (1,)), ((), ())), preferred_element_type=f32)

    def attend(q, k, vt, mask):
        s = scores_t(k, q)
        tail = jnp.where(mask, s[-QTILE:], -jnp.inf)
        s = tail if s.shape[0] == QTILE else jnp.concatenate([s[:-QTILE], tail], axis=0)
        m = jnp.max(s, axis=0, keepdims=True)
        e = jnp.exp(s - m)
        l = jnp.sum(e, axis=0, keepdims=True)
        o = jnp.dot(vt, e.astype(bf16), preferred_element_type=f32)
        return m, l, o

    tri = lax.broadcasted_iota(jnp.int32, (QTILE, QTILE), 0) <= lax.broadcasted_iota(
        jnp.int32, (QTILE, QTILE), 1
    )

    def lanes_of(p):
        return pl.ds(pl.multiple_of(p * LANES, LANES), LANES)

    def of_head(p, side):
        head = 2 * p + side
        return pl.ds(head, 1), pl.ds(pl.multiple_of(head * HEAD_DIM, HEAD_DIM), HEAD_DIM)

    def local(p):
        cols = lanes_of(p)
        for i in range(rows // QTILE):
            here = slice(i * QTILE, (i + 1) * QTILE)
            keys = slice(0, (i + 1) * QTILE)
            q, k = q_s[here, cols], k_s[keys, cols]
            for side in range(2):
                line, wide = of_head(p, side)
                m, l, o = attend(one_head(q, side), k, vt_s[wide, keys], tri)
                mx[line, here] = m
                sm[line, here] = l
                acc[wide, here] = o

    def throttled(act):
        @pl.when(me + 2 < n)
        def _():
            for which in range(2):
                for offset in range(n - 1, 0, -1):
                    @to(offset)
                    def _():
                        act(offset, which)

    def start_held(offset, which):
        kv_copy(offset, 1, which).start()

    pl.loop(0, pairs // 2)(local)
    throttled(start_held)
    pl.loop(pairs // 2, pairs)(local)

    def move_on(offset, which):
        kv_copy(offset, 1, which).wait_send()
        kv_copy(offset, 2, which).start()

    def arrive(g, which, count):
        for offset in range(1, count + 1):
            kv_copy(offset, g, which).wait_recv()

    def weigh(p, count):
        far = count * foreign_rows
        for i in range(rows // QTILE):
            here = slice(i * QTILE, (i + 1) * QTILE)
            for side in range(2):
                line, _ = of_head(p, side)
                m, l = mx[line, here], sm[line, here]
                if count:
                    s = scores_t(got_k[p, :far, :], one_head(q_s[here, lanes_of(p)], side))
                    t = jnp.maximum(m, jnp.max(s, axis=0, keepdims=True))
                    e = jnp.exp(s - t)
                    k = jnp.exp(m - t)
                    l = l * k + jnp.sum(e, axis=0, keepdims=True)
                    far_e[side, :far, here] = e.astype(bf16)
                    m = t
                r = 1.0 / l
                inv[line, here] = r
                keep_inv[line, here] = k * r if count else r
                lse_ref[0, line, here] = m + jnp.log(l)

    theirs = pl.ds(pl.multiple_of((1 - core) * half, half), half)
    mine = pl.ds(pl.multiple_of(core * half, half), half)

    def blend(p, count, send=None):
        far = count * foreign_rows
        for cols in (theirs, mine):
            heads = []
            for side in range(2):
                line, wide = of_head(p, side)
                o = acc[wide, cols] * keep_inv[line, cols]
                if count:
                    vt = got_v[p, side * HEAD_DIM:(side + 1) * HEAD_DIM, :far]
                    o = o + jnp.dot(vt, far_e[side, :far, cols], preferred_element_type=f32) * inv[line, cols]
                heads.append(o.astype(bf16))
            block = jnp.concatenate(heads, axis=0).T
            if cols is theirs:
                att_send[p] = block
                if send is not None:
                    att_copy(send).start()
            else:
                att[0, p] = block

    def each_count(act):
        for count in range(n):
            @pl.when(me == count)
            def _():
                act(count)

    def early(count):
        arrive(0, 0, count)
        arrive(0, 1, count)

        @pl.loop(0, early_pairs)
        def _(p):
            weigh(p, count)
            blend(p, count)

    def middle(count):
        arrive(1, 0, count)
        weigh(last - 1, count)
        arrive(1, 1, count)
        blend(last - 1, count, 1)

    def weigh_last(count):
        arrive(2, 0, count)
        weigh(last, count)

    def blend_last(count):
        arrive(2, 1, count)
        blend(last, count, 2)

    each_count(early)
    att_copy(0).start()
    throttled(move_on)
    each_count(middle)

    wo_own.wait()
    wo_far.wait_recv()
    last_wo_ref[...] = wo[last].reshape(2 * LANES, depth)
    each_count(weigh_last)

    each_count(blend_last)
    for g in range(2):
        att_copy(g).wait_recv()
    step = depth // 4
    for c in range(4):
        cols = slice(c * step, (c + 1) * step)
        rows_of = jnp.concatenate([att[side, p] for p in range(last) for side in range(2)], axis=1)
        out_ref[:, cols] = jnp.dot(
            rows_of, wo[:last, :, :, cols].reshape(2 * last * LANES, step), preferred_element_type=f32
        )

    att_copy(2).wait_recv()
    last_att_ref[...] = jnp.concatenate([att[0, last], att[1, last]], axis=1)

    for g in range(3):
        att_copy(g).wait_send()
    wo_far.wait_send()
    for offset in range(1, n):
        @pl.when(me >= offset)
        def _():
            ask_copy(offset).wait_send()

        @to(offset)
        def _():
            for which in range(2):
                for g in (0, 2):
                    kv_copy(offset, g, which).wait_send()

                @pl.when(me + 2 >= n)
                def _():
                    kv_copy(offset, 1, which).wait_send()


def final_kernel(part_ref, att_ref, wo_ref, lse_ref, mixed_hbm, lse_hbm, out, sem):
    lse_copy = pltpu.make_async_copy(lse_ref, lse_hbm, sem.at[1])
    lse_copy.start()
    step = out.shape[1] // 4
    for c in range(4):
        cols = slice(c * step, (c + 1) * step)
        out[:, cols] = (
            part_ref[:, cols] + jnp.dot(att_ref[...], wo_ref[:, cols], preferred_element_type=jnp.float32)
        ).astype(out.dtype)
        pltpu.make_async_copy(out.at[:, cols], mixed_hbm.at[0, :, cols], sem.at[0]).start()
    pltpu.make_async_copy(out, mixed_hbm.at[0], sem.at[0]).wait()
    lse_copy.wait()


def on_device_fused(n, tokens, w_query, w_key, w_value, w_out, chosen):
    _, rows, model = tokens.shape
    width = w_query.shape[1]
    depth = w_out.shape[1]
    blocks, picks = chosen.shape[1:]
    foreign_rows = CAPACITY * BLOCK
    heads = width // HEAD_DIM
    pairs = width // LANES
    half = rows // 2
    bf16, f32 = jnp.bfloat16, jnp.float32
    in_hbm = pl.BlockSpec(memory_space=pltpu.HBM)
    in_vmem = pl.BlockSpec(memory_space=pltpu.VMEM)
    dma = pltpu.SemaphoreType.DMA
    operands = [
        pltpu.with_memory_space_constraint(a, pltpu.HBM)
        for a in (tokens, w_query, w_key, w_value, w_out.reshape(pairs, LANES, depth), chosen)
    ]
    parts = pl.pallas_call(
        functools.partial(fused_kernel, n),
        out_shape=(
            pltpu.VMEM((half, depth), f32),
            pltpu.VMEM((half, 2 * LANES), bf16),
            pltpu.VMEM((2 * LANES, depth), bf16),
            pltpu.VMEM((1, heads, rows), f32),
        ),
        in_specs=[in_hbm] * 6,
        out_specs=(in_vmem,) * 4,
        scratch_shapes=[
            pltpu.VMEM((rows, model), bf16),
            pltpu.VMEM((model, width), bf16),
            pltpu.VMEM((model, width), bf16),
            pltpu.VMEM((model, width), bf16),
            pltpu.VMEM((pairs, 2, LANES, depth), bf16),
            pltpu.VMEM((1, blocks, picks), jnp.int32),
            pltpu.VMEM((rows, width), bf16),
            pltpu.VMEM((rows, width), bf16),
            pltpu.VMEM((width, rows), bf16),
            pltpu.VMEM((n - 1, foreign_rows, rows), bf16),
            pltpu.VMEM((n - 1, pairs, foreign_rows, LANES), bf16),
            pltpu.VMEM((n - 1, pairs, LANES, foreign_rows), bf16),
            pltpu.VMEM((pairs, (n - 1) * foreign_rows, LANES), bf16),
            pltpu.VMEM((pairs, LANES, (n - 1) * foreign_rows), bf16),
            pltpu.VMEM((n - 1, 1, blocks, picks), jnp.int32),
            pltpu.VMEM((width, rows), f32),
            pltpu.VMEM((heads, rows), f32),
            pltpu.VMEM((heads, rows), f32),
            pltpu.VMEM((heads, rows), f32),
            pltpu.VMEM((heads, rows), f32),
            pltpu.VMEM((2, (n - 1) * foreign_rows, rows), bf16),
            pltpu.VMEM((2, pairs, half, LANES), bf16),
            pltpu.VMEM((pairs, half, LANES), bf16),
            dma((4,)),
            dma((2, 2)),
            dma((n - 1,)),
            dma((n - 1,)),
            dma((2, n - 1, 3)),
            dma((2, n - 1, 3)),
            dma((3,)),
            dma((3,)),
            dma,
            dma,
        ],
        compiler_params=pltpu.CompilerParams(
            collective_id=0, has_side_effects=True, vmem_limit_bytes=40 * 1024 * 1024
        ),
    )(*operands)
    return pl.pallas_call(
        final_kernel,
        out_shape=(
            jax.ShapeDtypeStruct((1, half, depth), bf16),
            jax.ShapeDtypeStruct((1, heads, rows), f32),
        ),
        in_specs=[in_vmem] * 4,
        out_specs=(in_hbm, in_hbm),
        scratch_shapes=[pltpu.VMEM((half, depth), bf16), dma((2,))],
        compiler_params=pltpu.CompilerParams(vmem_limit_bytes=4 * 1024 * 1024),
    )(*[pltpu.with_memory_space_constraint(a, pltpu.VMEM) for a in parts])


def on_device(tokens, w_query, w_key, w_value, w_out, chosen):
    n, cores = lax.axis_size("kv"), lax.axis_size("tp")
    rows, width = tokens.shape[1], w_query.shape[1]
    blocks, picks = chosen.shape[1:]
    full_rows = blocks - 1 + CAPACITY * (n - 1) <= picks - 1
    fits = rows == 2 * QTILE and width == 2 * STEP and blocks >= 3 * CAPACITY
    if full_rows and fits and cores == 2 and n > 1:
        return on_device_fused(n, tokens, w_query, w_key, w_value, w_out, chosen)
    return on_device_general(tokens, w_query, w_key, w_value, w_out, chosen)


def solution(mesh):
    return jax.shard_map(
        on_device,
        mesh=mesh,
        in_specs=(
            P("dp", "kv", None),
            P(None, "tp"),
            P(None, "tp"),
            P(None, "tp"),
            P("tp", None),
            P("dp", "kv", None),
        ),
        out_specs=(P("dp", ("kv", "tp"), None), P("dp", "tp", "kv")),
        check_vma=False,
    )
```

```python
import functools

import jax
import jax.numpy as jnp
from jax import lax
from jax.experimental import pallas as pl
from jax.experimental.pallas import tpu as pltpu
from jax.sharding import PartitionSpec as P

HEAD_DIM = 64
BLOCK = 64


def on_device_general(tokens, w_query, w_key, w_value, w_out, chosen):
    inputs = tokens[0]
    listed = chosen[0]
    tok_rows = inputs.shape[0]
    queries = jnp.dot(inputs, w_query, preferred_element_type=jnp.float32).astype(jnp.bfloat16)
    keys_local = jnp.dot(inputs, w_key, preferred_element_type=jnp.float32).astype(jnp.bfloat16)
    values_local = jnp.dot(inputs, w_value, preferred_element_type=jnp.float32).astype(jnp.bfloat16)
    width = queries.shape[1]
    head_count = width // HEAD_DIM
    span_blocks = tok_rows // BLOCK
    query_count, picks = listed.shape
    myself = lax.axis_index("kv")
    valid = listed >= 0
    key_blocks = keys_local.reshape(span_blocks, BLOCK, width)
    value_blocks = values_local.reshape(span_blocks, BLOCK, width)
    kv_count = lax.axis_size("kv")
    capacity = max(1, min(2, span_blocks // 3))
    owners = jnp.where(valid, listed // span_blocks, myself)
    within = jnp.where(valid, listed % span_blocks, 0)
    foreign = valid & (owners != myself)
    owner_iota = jnp.arange(kv_count, dtype=jnp.int32)
    within_iota = jnp.arange(span_blocks, dtype=jnp.int32)
    hits = (
        (owners[:, :, None, None] == owner_iota[:, None])
        & (within[:, :, None, None] == within_iota[None, :])
        & foreign[:, :, None, None]
    )
    needed = jnp.any(hits, axis=(0, 1))
    order_rank = jnp.cumsum(needed.astype(jnp.int32), axis=1) - 1
    matches = needed[:, None, :] & (
        order_rank[:, None, :] == jnp.arange(capacity, dtype=jnp.int32)[None, :, None]
    )
    wanted = jnp.where(
        jnp.any(matches, axis=2), jnp.sum(matches.astype(jnp.int32) * within_iota, axis=2), -1
    )
    asked = lax.all_to_all(wanted, "kv", split_axis=0, concat_axis=0, tiled=True)
    present = (asked >= 0)[:, :, None, None]
    picked = jnp.clip(asked, 0, span_blocks - 1)
    zero_block = jnp.zeros((), jnp.bfloat16)
    send_keys = jnp.where(present, key_blocks[picked], zero_block)
    send_values = jnp.where(present, value_blocks[picked], zero_block)
    got_keys, got_values = (
        lax.all_to_all(send_keys, "kv", split_axis=0, concat_axis=0, tiled=True),
        lax.all_to_all(send_values, "kv", split_axis=0, concat_axis=0, tiled=True),
    )
    pool_keys = jnp.concatenate([key_blocks, got_keys.reshape(-1, BLOCK, width)], axis=0)
    pool_values = jnp.concatenate([value_blocks, got_values.reshape(-1, BLOCK, width)], axis=0)
    slot_rank = jnp.sum(hits.astype(jnp.int32) * order_rank[None, None], axis=(2, 3))
    slots = jnp.where(foreign, span_blocks + owners * capacity + slot_rank, within)
    keys_sel = pool_keys[slots].reshape(query_count, picks, BLOCK, head_count, HEAD_DIM)
    values_sel = pool_values[slots].reshape(query_count, picks, BLOCK, head_count, HEAD_DIM)
    query_blocks = queries.reshape(query_count, BLOCK, head_count, HEAD_DIM)
    scores = jnp.einsum(
        "nqhd,nskhd->nhqsk", query_blocks, keys_sel, preferred_element_type=jnp.float32
    ) * HEAD_DIM ** (-0.5)
    offsets = jnp.arange(BLOCK, dtype=jnp.int32)
    key_pos = listed[:, :, None] * BLOCK + offsets[None, None, :]
    query_pos = (myself * span_blocks + jnp.arange(query_count, dtype=jnp.int32))[
        :, None
    ] * BLOCK + offsets[None, :]
    allowed = valid[:, None, :, None] & (key_pos[:, None, :, :] <= query_pos[:, :, None, None])
    scores = jnp.where(allowed[:, None], scores, -jnp.inf)
    row_max = jnp.max(scores, axis=(3, 4), keepdims=True)
    exp_terms = jnp.exp(scores - row_max)
    row_sum = jnp.sum(exp_terms, axis=(3, 4), keepdims=True)
    weights = (exp_terms / row_sum).astype(jnp.bfloat16)
    attended = jnp.einsum(
        "nhqsk,nskhd->nqhd", weights, values_sel, preferred_element_type=jnp.float32
    )
    attended = attended.astype(jnp.bfloat16).reshape(tok_rows, width)
    log_sums = (row_max + jnp.log(row_sum))[:, :, :, 0, 0]
    log_sums = jnp.transpose(log_sums, (1, 0, 2)).reshape(head_count, tok_rows)
    mixed = lax.psum_scatter(
        jnp.dot(attended, w_out, preferred_element_type=jnp.float32).astype(jnp.bfloat16),
        "tp",
        scatter_dimension=0,
        tiled=True,
    )
    return (mixed[None], log_sums[None])


CAPACITY = 2
LANES = 128
QTILE = 256
STEP = 256


def fused_kernel(
    n, tokens_hbm, wq_hbm, wk_hbm, wv_hbm, wo_hbm, chosen_hbm, out_ref, last_att_ref, last_wo_ref, lse_ref,
    x, wq, wk, wv, wo, chosen_ref, q_s, k_s, vt_s, hot, send_k, send_v, got_k, got_v, asked,
    acc, mx, sm, inv, keep_inv, far_e, att, att_send,
    load_sem, w_sem, ask_send, ask_recv, held_send, bulk_send, kv_recv, att_sem_s, att_sem_r, wo_send, wo_recv,
):
    me = lax.axis_index("kv")
    core = lax.axis_index("tp")
    rows, width = q_s.shape
    depth = wo.shape[3]
    half = rows // 2
    blocks = rows // BLOCK
    pairs = width // LANES
    chunks = width // STEP
    per_chunk = STEP // LANES
    foreign_rows = CAPACITY * BLOCK
    last = pairs - 1
    early_pairs = pairs - 2
    bf16, f32 = jnp.bfloat16, jnp.float32
    mesh_ids = pl.DeviceIdType.MESH

    def part(c):
        return slice(c * STEP, (c + 1) * STEP)

    load_chosen = pltpu.make_async_copy(chosen_hbm, chosen_ref, load_sem.at[0])
    load_x = pltpu.make_async_copy(tokens_hbm.at[0], x, load_sem.at[1])
    load_q = pltpu.make_async_copy(wq_hbm, wq, load_sem.at[0])
    weights = ((wk_hbm, wk), (wv_hbm, wv))

    def load_w(which, c):
        src, dst = weights[which]
        slot = ((0, 2), (1, 0))[which][c]
        return pltpu.make_async_copy(src.at[:, part(c)], dst.at[:, part(c)], w_sem.at[slot])

    wo_own = pltpu.make_async_copy(wo_hbm, wo.at[:, 0], load_sem.at[1])
    wo_far = pltpu.make_async_remote_copy(
        src_ref=wo_hbm, dst_ref=wo.at[:, 1], send_sem=wo_send, recv_sem=wo_recv,
        device_id={"tp": 1 - core}, device_id_type=mesh_ids,
    )

    load_chosen.start()
    load_x.start()
    load_w(0, 0).start()

    barrier = pltpu.get_barrier_semaphore()
    for offset in range(1, n):
        @pl.when(me + offset < n)
        def _():
            pl.semaphore_signal(barrier, inc=1, device_id={"kv": me + offset}, device_id_type=mesh_ids)
    pl.semaphore_signal(barrier, inc=1, device_id={"tp": 1 - core}, device_id_type=mesh_ids)

    def ask_copy(offset):
        return pltpu.make_async_remote_copy(
            src_ref=chosen_ref, dst_ref=asked.at[offset - 1],
            send_sem=ask_send, recv_sem=ask_recv.at[offset - 1],
            device_id={"kv": lax.rem(me + n - offset, n)}, device_id_type=mesh_ids,
        )

    def kv_copy(offset, g, which):
        far = pl.ds((offset - 1) * foreign_rows, foreign_rows)
        group = pl.ds(0, early_pairs) if g == 0 else pl.ds(early_pairs + g - 1, 1)
        return pltpu.make_async_remote_copy(
            src_ref=(send_k, send_v)[which].at[offset - 1, group],
            dst_ref=got_k.at[group, far, :] if which == 0 else got_v.at[group, :, far],
            send_sem=held_send.at[which, offset - 1] if g == 1 else bulk_send.at[which, g // 2],
            recv_sem=kv_recv.at[which, g],
            device_id={"kv": lax.rem(me + offset, n)}, device_id_type=mesh_ids,
        )

    def att_copy(g):
        group = pl.ds(0, early_pairs) if g == 0 else pl.ds(early_pairs + g - 1, 1)
        return pltpu.make_async_remote_copy(
            src_ref=att_send.at[group], dst_ref=att.at[1, group],
            send_sem=att_sem_s.at[g], recv_sem=att_sem_r.at[g],
            device_id={"tp": 1 - core}, device_id_type=mesh_ids,
        )

    load_chosen.wait()
    pl.semaphore_wait(barrier, me + 1)
    for offset in range(1, n):
        @pl.when(me >= offset)
        def _():
            ask_copy(offset).start()
    load_w(1, 0).start()
    load_w(0, 1).start()

    def project_k(c):
        load_w(0, c).wait()
        cols = part(c)
        for r in (slice(0, half), slice(half, rows)):
            k_s[r, cols] = jnp.dot(x[r, :], wk[:, cols], preferred_element_type=f32).astype(bf16)

    def project_v(c):
        load_w(1, c).wait()
        cols = part(c)
        for r in (slice(0, half), slice(half, rows)):
            y = jnp.dot(x[r, :], wv[:, cols], preferred_element_type=f32).astype(bf16)
            vt_s[cols, r] = y.T

    def project_q():
        load_q.wait()

        @pl.loop(0, chunks)
        def _(c):
            cols = pl.ds(pl.multiple_of(c * STEP, STEP), STEP)
            y = jnp.dot(x[...], wq[:, cols], preferred_element_type=f32).astype(bf16)
            q_s[:, cols] = y * jnp.asarray(HEAD_DIM ** (-0.5), bf16)

    def pick(offset):
        ask_copy(offset).wait_recv()
        row = asked[offset - 1, 0, 0:1, :]
        inside = (row >= me * blocks) & (row < (me + 1) * blocks)
        low = jnp.min(jnp.where(inside, row, (me + 1) * blocks - 1), axis=1, keepdims=True)
        high = jnp.max(jnp.where(inside, row, me * blocks), axis=1, keepdims=True)
        low, high = (low - me * blocks) * BLOCK, (high - me * blocks - 1) * BLOCK
        place = lax.broadcasted_iota(jnp.int32, (foreign_rows, rows), 0)
        column = lax.broadcasted_iota(jnp.int32, (foreign_rows, rows), 1)
        want = place + jnp.where(place < BLOCK, low, high)
        hot[offset - 1] = (column == want).astype(f32).astype(bf16)

    def gather_and_send(offset, c, kinds):
        for which in kinds:
            if which == 0:
                y = jnp.dot(hot[offset - 1], k_s[:, part(c)], preferred_element_type=f32).astype(bf16)
            else:
                y = lax.dot_general(
                    vt_s[part(c), :], hot[offset - 1], (((1,), (1,)), ((), ())), preferred_element_type=f32
                ).astype(bf16)
            for i in range(per_chunk):
                here = slice(i * LANES, (i + 1) * LANES)
                if which == 0:
                    send_k[offset - 1, c * per_chunk + i] = y[:, here]
                else:
                    send_v[offset - 1, c * per_chunk + i] = y[here, :]
            if c * per_chunk < early_pairs:
                kv_copy(offset, 0, which).start()
        if c == chunks - 1:
            @pl.when(me + 2 >= n)
            def _():
                for g in (1, 2):
                    for which in kinds:
                        kv_copy(offset, g, which).start()

    def to(offset):
        return pl.when(me + offset < n)

    load_x.wait()
    project_k(0)

    @pl.when((me >= 1) & (me + 1 < n))
    def _():
        pick(1)
        gather_and_send(1, 0, (0,))

    load_w(1, 1).start()
    load_q.start()
    project_v(0)

    @pl.when((me >= 1) & (me + 1 < n))
    def _():
        gather_and_send(1, 0, (1,))

    project_k(1)
    for offset in range(2, n):
        @pl.when((me >= 1) & (me + offset < n))
        def _():
            pick(offset)
            gather_and_send(offset, 0, (0, 1))

    project_v(1)

    @pl.when(me >= 1)
    def _():
        for offset in range(1, n):
            @to(offset)
            def _():
                gather_and_send(offset, 1, (0, 1))

    wo_own.start()
    wo_far.start()
    project_q()

    @pl.when(me == 0)
    def _():
        for offset in range(1, n):
            pick(offset)
            gather_and_send(offset, 0, (0, 1))
        for offset in range(1, n):
            gather_and_send(offset, 1, (0, 1))

    first = lax.broadcasted_iota(jnp.int32, (QTILE, LANES), 1) < HEAD_DIM
    zero = jnp.zeros((), bf16)

    def one_head(q, side):
        return jnp.where(first, q, zero) if side == 0 else jnp.where(first, zero, q)

    def scores_t(k, q):
        return lax.dot_general(k, q, (((1,), (1,)), ((), ())), preferred_element_type=f32)

    def attend(q, k, vt, mask):
        s = scores_t(k, q)
        tail = jnp.where(mask, s[-QTILE:], -jnp.inf)
        s = tail if s.shape[0] == QTILE else jnp.concatenate([s[:-QTILE], tail], axis=0)
        m = jnp.max(s, axis=0, keepdims=True)
        e = jnp.exp(s - m)
        l = jnp.sum(e, axis=0, keepdims=True)
        o = jnp.dot(vt, e.astype(bf16), preferred_element_type=f32)
        return m, l, o

    tri = lax.broadcasted_iota(jnp.int32, (QTILE, QTILE), 0) <= lax.broadcasted_iota(
        jnp.int32, (QTILE, QTILE), 1
    )

    def lanes_of(p):
        return pl.ds(pl.multiple_of(p * LANES, LANES), LANES)

    def of_head(p, side):
        head = 2 * p + side
        return pl.ds(head, 1), pl.ds(pl.multiple_of(head * HEAD_DIM, HEAD_DIM), HEAD_DIM)

    def local(p):
        cols = lanes_of(p)
        for i in range(rows // QTILE):
            here = slice(i * QTILE, (i + 1) * QTILE)
            keys = slice(0, (i + 1) * QTILE)
            q, k = q_s[here, cols], k_s[keys, cols]
            for side in range(2):
                line, wide = of_head(p, side)
                m, l, o = attend(one_head(q, side), k, vt_s[wide, keys], tri)
                mx[line, here] = m
                sm[line, here] = l
                acc[wide, here] = o

    def throttled(act):
        @pl.when(me + 2 < n)
        def _():
            for which in range(2):
                for offset in range(n - 1, 0, -1):
                    @to(offset)
                    def _():
                        act(offset, which)

    def start_held(offset, which):
        kv_copy(offset, 1, which).start()

    pl.loop(0, pairs // 2)(local)
    throttled(start_held)
    pl.loop(pairs // 2, pairs)(local)

    def move_on(offset, which):
        kv_copy(offset, 1, which).wait_send()
        kv_copy(offset, 2, which).start()

    def arrive(g, which, count):
        if count:
            far = pl.ds(0, count * foreign_rows)
            group = pl.ds(0, early_pairs) if g == 0 else pl.ds(early_pairs + g - 1, 1)
            landed = got_k.at[group, far, :] if which == 0 else got_v.at[group, :, far]
            pltpu.make_async_copy(landed, landed, kv_recv.at[which, g]).wait()

    def weigh(p, count):
        far = count * foreign_rows
        for i in range(rows // QTILE):
            here = slice(i * QTILE, (i + 1) * QTILE)
            for side in range(2):
                line, _ = of_head(p, side)
                m, l = mx[line, here], sm[line, here]
                if count:
                    s = scores_t(got_k[p, :far, :], one_head(q_s[here, lanes_of(p)], side))
                    t = jnp.maximum(m, jnp.max(s, axis=0, keepdims=True))
                    e = jnp.exp(s - t)
                    k = jnp.exp(m - t)
                    l = l * k + jnp.sum(e, axis=0, keepdims=True)
                    far_e[side, :far, here] = e.astype(bf16)
                    m = t
                r = 1.0 / l
                inv[line, here] = r
                keep_inv[line, here] = k * r if count else r
                lse_ref[0, line, here] = m + jnp.log(l)

    theirs = pl.ds(pl.multiple_of((1 - core) * half, half), half)
    mine = pl.ds(pl.multiple_of(core * half, half), half)

    def blend(p, count, send=None):
        far = count * foreign_rows
        for cols in (theirs, mine):
            heads = []
            for side in range(2):
                line, wide = of_head(p, side)
                o = acc[wide, cols] * keep_inv[line, cols]
                if count:
                    vt = got_v[p, side * HEAD_DIM:(side + 1) * HEAD_DIM, :far]
                    o = o + jnp.dot(vt, far_e[side, :far, cols], preferred_element_type=f32) * inv[line, cols]
                heads.append(o.astype(bf16))
            block = jnp.concatenate(heads, axis=0).T
            if cols is theirs:
                att_send[p] = block
                if send is not None:
                    att_copy(send).start()
            else:
                att[0, p] = block

    def each_count(act):
        for count in range(n):
            @pl.when(me == count)
            def _():
                act(count)

    def early(count):
        arrive(0, 0, count)
        arrive(0, 1, count)

        @pl.loop(0, early_pairs)
        def _(p):
            weigh(p, count)
            blend(p, count)

    def middle(count):
        arrive(1, 0, count)
        weigh(last - 1, count)
        arrive(1, 1, count)
        blend(last - 1, count, 1)

    def weigh_last(count):
        arrive(2, 0, count)
        weigh(last, count)

    def blend_last(count):
        arrive(2, 1, count)
        blend(last, count, 2)

    each_count(early)
    att_copy(0).start()
    throttled(move_on)
    each_count(middle)

    wo_own.wait()
    wo_far.wait_recv()
    last_wo_ref[...] = wo[last].reshape(2 * LANES, depth)
    each_count(weigh_last)

    each_count(blend_last)
    for g in range(2):
        att_copy(g).wait_recv()
    step = depth // 4
    for c in range(4):
        cols = slice(c * step, (c + 1) * step)
        rows_of = jnp.concatenate([att[side, p] for p in range(last) for side in range(2)], axis=1)
        out_ref[:, cols] = jnp.dot(
            rows_of, wo[:last, :, :, cols].reshape(2 * last * LANES, step), preferred_element_type=f32
        )

    att_copy(2).wait_recv()
    last_att_ref[...] = jnp.concatenate([att[0, last], att[1, last]], axis=1)

    for g in range(3):
        att_copy(g).wait_send()
    wo_far.wait_send()
    for count in range(1, n):
        @pl.when(me == count)
        def _():
            asks = asked.at[pl.ds(0, count)]
            pltpu.make_async_copy(asks, asks, ask_send).wait()

        @pl.when(me + count == n - 1)
        def _():
            for which in range(2):
                sent = (send_k, send_v)[which]
                for g, group in ((0, pl.ds(0, early_pairs)), (1, pl.ds(last, 1))):
                    gone = sent.at[pl.ds(0, count), group]
                    pltpu.make_async_copy(gone, gone, bulk_send.at[which, g]).wait()

    @pl.when(me + 2 == n)
    def _():
        for which in range(2):
            kv_copy(1, 1, which).wait_send()


def final_kernel(part_ref, att_ref, wo_ref, lse_ref, mixed_hbm, lse_hbm, out, sem):
    lse_copy = pltpu.make_async_copy(lse_ref, lse_hbm, sem.at[1])
    lse_copy.start()
    step = out.shape[1] // 4
    for c in range(4):
        cols = slice(c * step, (c + 1) * step)
        out[:, cols] = (
            part_ref[:, cols] + jnp.dot(att_ref[...], wo_ref[:, cols], preferred_element_type=jnp.float32)
        ).astype(out.dtype)
        pltpu.make_async_copy(out.at[:, cols], mixed_hbm.at[0, :, cols], sem.at[0]).start()
    pltpu.make_async_copy(out, mixed_hbm.at[0], sem.at[0]).wait()
    lse_copy.wait()


def on_device_fused(n, tokens, w_query, w_key, w_value, w_out, chosen):
    _, rows, model = tokens.shape
    width = w_query.shape[1]
    depth = w_out.shape[1]
    blocks, picks = chosen.shape[1:]
    foreign_rows = CAPACITY * BLOCK
    heads = width // HEAD_DIM
    pairs = width // LANES
    half = rows // 2
    bf16, f32 = jnp.bfloat16, jnp.float32
    in_hbm = pl.BlockSpec(memory_space=pltpu.HBM)
    in_vmem = pl.BlockSpec(memory_space=pltpu.VMEM)
    dma = pltpu.SemaphoreType.DMA
    operands = [
        pltpu.with_memory_space_constraint(a, pltpu.HBM)
        for a in (tokens, w_query, w_key, w_value, w_out.reshape(pairs, LANES, depth), chosen)
    ]
    parts = pl.pallas_call(
        functools.partial(fused_kernel, n),
        out_shape=(
            pltpu.VMEM((half, depth), f32),
            pltpu.VMEM((half, 2 * LANES), bf16),
            pltpu.VMEM((2 * LANES, depth), bf16),
            pltpu.VMEM((1, heads, rows), f32),
        ),
        in_specs=[in_hbm] * 6,
        out_specs=(in_vmem,) * 4,
        scratch_shapes=[
            pltpu.VMEM((rows, model), bf16),
            pltpu.VMEM((model, width), bf16),
            pltpu.VMEM((model, width), bf16),
            pltpu.VMEM((model, width), bf16),
            pltpu.VMEM((pairs, 2, LANES, depth), bf16),
            pltpu.VMEM((1, blocks, picks), jnp.int32),
            pltpu.VMEM((rows, width), bf16),
            pltpu.VMEM((rows, width), bf16),
            pltpu.VMEM((width, rows), bf16),
            pltpu.VMEM((n - 1, foreign_rows, rows), bf16),
            pltpu.VMEM((n - 1, pairs, foreign_rows, LANES), bf16),
            pltpu.VMEM((n - 1, pairs, LANES, foreign_rows), bf16),
            pltpu.VMEM((pairs, (n - 1) * foreign_rows, LANES), bf16),
            pltpu.VMEM((pairs, LANES, (n - 1) * foreign_rows), bf16),
            pltpu.VMEM((n - 1, 1, blocks, picks), jnp.int32),
            pltpu.VMEM((width, rows), f32),
            pltpu.VMEM((heads, rows), f32),
            pltpu.VMEM((heads, rows), f32),
            pltpu.VMEM((heads, rows), f32),
            pltpu.VMEM((heads, rows), f32),
            pltpu.VMEM((2, (n - 1) * foreign_rows, rows), bf16),
            pltpu.VMEM((2, pairs, half, LANES), bf16),
            pltpu.VMEM((pairs, half, LANES), bf16),
            dma((2,)),
            dma((3,)),
            dma,
            dma((n - 1,)),
            dma((2, n - 1)),
            dma((2, 2)),
            dma((2, 3)),
            dma((3,)),
            dma((3,)),
            dma,
            dma,
        ],
        compiler_params=pltpu.CompilerParams(
            collective_id=0, has_side_effects=True, vmem_limit_bytes=40 * 1024 * 1024
        ),
    )(*operands)
    return pl.pallas_call(
        final_kernel,
        out_shape=(
            jax.ShapeDtypeStruct((1, half, depth), bf16),
            jax.ShapeDtypeStruct((1, heads, rows), f32),
        ),
        in_specs=[in_vmem] * 4,
        out_specs=(in_hbm, in_hbm),
        scratch_shapes=[pltpu.VMEM((half, depth), bf16), dma((2,))],
        compiler_params=pltpu.CompilerParams(vmem_limit_bytes=4 * 1024 * 1024),
    )(*[pltpu.with_memory_space_constraint(a, pltpu.VMEM) for a in parts])


def on_device(tokens, w_query, w_key, w_value, w_out, chosen):
    n, cores = lax.axis_size("kv"), lax.axis_size("tp")
    rows, width = tokens.shape[1], w_query.shape[1]
    blocks, picks = chosen.shape[1:]
    full_rows = blocks - 1 + CAPACITY * (n - 1) <= picks - 1
    fits = rows == 2 * QTILE and width == 2 * STEP and blocks >= 3 * CAPACITY
    if full_rows and fits and cores == 2 and n > 1:
        return on_device_fused(n, tokens, w_query, w_key, w_value, w_out, chosen)
    return on_device_general(tokens, w_query, w_key, w_value, w_out, chosen)


def solution(mesh):
    return jax.shard_map(
        on_device,
        mesh=mesh,
        in_specs=(
            P("dp", "kv", None),
            P(None, "tp"),
            P(None, "tp"),
            P(None, "tp"),
            P("tp", None),
            P("dp", "kv", None),
        ),
        out_specs=(P("dp", ("kv", "tp"), None), P("dp", "tp", "kv")),
        check_vma=False,
    )
```
